32 devices in a mesh: sp: 8 (over z, y), tp: 4 (over x, core).
Axes of the slice: x: 2, y: 2, z: 4, core: 2. Of those that a mesh axis runs over, the one named last changes fastest.
Arguments:
- tokens: bfloat16 [8192, 2048], P('sp', 'tp'), may hold values from -16 to 16
- mix_gain: float32 [2048], replicated, may hold values from 0.1 to 1.9
- query_weight: bfloat16 [2048, 1024], P(None, 'tp'), may hold values from -0.125 to 0.125
- key_weight: bfloat16 [2048, 1024], P(None, 'tp'), may hold values from -0.125 to 0.125
- value_weight: bfloat16 [2048, 1024], P(None, 'tp'), may hold values from -0.125 to 0.125
- outer_gate_weight: bfloat16 [2048, 1024], P(None, 'tp'), may hold values from -0.125 to 0.125
- inner_gate_weight: bfloat16 [2048, 1024], P(None, 'tp'), may hold values from -0.125 to 0.125
- conv_input_weight: bfloat16 [2048, 1024], P(None, 'tp'), may hold values from -0.125 to 0.125
- query_gain: float32 [64], replicated, may hold values from 0.6 to 10
- key_gain: float32 [64], replicated, may hold values from 0.6 to 10
- gate_totals: float32 [8192, 16], P('sp', 'tp'), may hold values from -2048 to 0, as said below
- conv_taps: float32 [3, 1024], P(None, 'tp'), may hold values from -3 to 3
- attn_out_gain: float32 [1024], P('tp'), may hold values from 0.1 to 1.9
- conv_out_gain: float32 [1024], P('tp'), may hold values from 0.1 to 1.9
- attn_out_weight: bfloat16 [1024, 2048], P('tp'), may hold values from -0.125 to 0.125
- conv_out_weight: bfloat16 [1024, 2048], P('tp'), may hold values from -0.125 to 0.125
Outputs:
- mixed: bfloat16 [8192, 2048], P(('sp', 'tp'))
The draws below stay inside these ranges and needn't reach their ends.
Inputs may be any that keep to these rules, and one draw needn't show every extreme that they name: `gate_totals`: in every head the values never rise from one position to the next.
All inputs are finite; a program needn't handle non-finite values.
Results may differ from the reference program's by a relative error of at most 0.015.
The reference program's roundings to bfloat16 on the way count: a program that leaves them out, or rounds other values in their place, can miss the bound.
Values may be sent and summed in bfloat16 or wider, within the bound.
A program may use at most 64 MiB of HBM per device.

```python
import math
import jax
import jax.numpy as jnp
from jax import lax

D = 2048
HEAD_DIM = 64
ATTENTION_HEADS = 16
CONV_K = 3
TOK_DEV = 1024
ATTN_WIDTH = 1024
CONV_WIDTH = 1024
SEQUENCE_TOKENS = 8192
N_TP = 4


def draw_tokens(key, part):
    random_subkeys = jax.random.split(jax.random.fold_in(key, 101), 2)
    column = jnp.arange(D, dtype=jnp.float32) / D
    column_scale = 0.5 * jnp.exp(math.log(4.0) * column) * jax.random.uniform(random_subkeys[1], (D,), jnp.float32, 0.7, 1.4)
    normal_part = jax.random.normal(random_subkeys[0], (SEQUENCE_TOKENS, D), jnp.float32)
    return jnp.clip(normal_part * column_scale, -16.0, 16.0).astype(jnp.bfloat16)


def focus_gain(key):
    gain = jax.random.uniform(key, (HEAD_DIM,), jnp.float32, 0.6, 1.4)
    return gain


def draw_query_gain(key, part):
    return focus_gain(jax.random.fold_in(key, 211))


def draw_key_gain(key, part):
    return focus_gain(jax.random.fold_in(key, 307))


def draw_gate_totals(key, part):
    random_subkeys = jax.random.split(jax.random.fold_in(key, 401), 7)
    order = jax.random.permutation(random_subkeys[0], ATTENTION_HEADS)
    fast_path = order < ATTENTION_HEADS // 2
    slow_total = jax.random.uniform(random_subkeys[1], (ATTENTION_HEADS,), jnp.float32, 0.15, 0.5)
    quick_reach = jnp.exp(jax.random.uniform(random_subkeys[2], (ATTENTION_HEADS,), jnp.float32, math.log(30.0), math.log(100.0)))
    base_rate = jnp.where(fast_path, 1.0 / quick_reach, slow_total / SEQUENCE_TOKENS)
    block_factor = jnp.exp(jax.random.uniform(random_subkeys[3], (SEQUENCE_TOKENS // TOK_DEV, 1), jnp.float32, math.log(0.5), math.log(2.0)))
    block_rate = jnp.repeat(block_factor, TOK_DEV, axis=0)
    jitter = jnp.exp(jax.random.uniform(random_subkeys[4], (SEQUENCE_TOKENS, ATTENTION_HEADS), jnp.float32, math.log(0.5), math.log(2.0)))
    per_step_loss = base_rate[None, :] * block_rate * jitter
    spike_position = jax.random.randint(random_subkeys[5], (2,), 0, SEQUENCE_TOKENS)
    spike_hit = jnp.any(jnp.arange(SEQUENCE_TOKENS)[:, None] == spike_position[None, :], axis=1)
    spike_loss = jax.random.uniform(random_subkeys[6], (SEQUENCE_TOKENS, ATTENTION_HEADS), jnp.float32, 0.22, 0.51)
    per_step_loss = per_step_loss + jnp.where(spike_hit[:, None] & jnp.logical_not(fast_path)[None, :], spike_loss, 0.0)
    return -jnp.cumsum(per_step_loss, axis=0)


def block_levels(stream_key, shape, cuts, low, top_value):
    level, own = 1.0, jax.random.fold_in(stream_key, 6)
    for position, shards_of in cuts:
        draws = jnp.exp(jax.random.uniform(jax.random.fold_in(own, position), (shards_of,), jnp.float32, low / len(cuts), top_value / len(cuts)))
        level = level * jnp.repeat(draws, shape[position] // shards_of).reshape([-1 if axis == position else 1 for axis in range(len(shape))])
    return level


def centred(stream_key, shape, deviation, most, cuts=(), kind=jnp.bfloat16):
    array = deviation * jax.random.normal(stream_key, shape, jnp.float32)
    if cuts:
        array = array * block_levels(stream_key, shape, cuts, -0.22, 0.18)
    return jnp.clip(array, -most, most).astype(kind)


def setup_inputs(seed: int = 0) -> dict:
    key_of = jax.random.split(jax.random.key(seed), 17)
    return {
        "tokens": draw_tokens(jax.random.fold_in(key_of[16], 71), 0),
        "mix_gain": jnp.clip(1.0 + 0.18 * jax.random.normal(key_of[1], (D,), jnp.float32), 0.1, 1.9),
        "query_weight": centred(key_of[2], (D, ATTN_WIDTH), D ** -0.5, 0.125, ((1, 4),)),
        "key_weight": centred(key_of[3], (D, ATTN_WIDTH), D ** -0.5, 0.125, ((1, 4),)),
        "value_weight": centred(key_of[4], (D, ATTN_WIDTH), D ** -0.5, 0.125, ((1, 4),)),
        "outer_gate_weight": centred(key_of[5], (D, CONV_WIDTH), D ** -0.5, 0.125, ((1, 4),)),
        "inner_gate_weight": centred(key_of[6], (D, CONV_WIDTH), D ** -0.5, 0.125, ((1, 4),)),
        "conv_input_weight": centred(key_of[7], (D, CONV_WIDTH), D ** -0.5, 0.125, ((1, 4),)),
        "query_gain": draw_query_gain(jax.random.fold_in(key_of[16], 71), 0),
        "key_gain": draw_key_gain(jax.random.fold_in(key_of[16], 71), 0),
        "gate_totals": draw_gate_totals(jax.random.fold_in(key_of[16], 71), 0),
        "conv_taps": centred(key_of[11], (CONV_K, CONV_WIDTH), 0.6, 3.0, ((1, 4),), jnp.float32),
        "attn_out_gain": jnp.clip(1.0 + 0.18 * jax.random.normal(key_of[12], (ATTN_WIDTH,), jnp.float32), 0.1, 1.9),
        "conv_out_gain": jnp.clip(1.0 + 0.18 * jax.random.normal(key_of[13], (CONV_WIDTH,), jnp.float32), 0.1, 1.9),
        "attn_out_weight": centred(key_of[14], (ATTN_WIDTH, D), (ATTN_WIDTH + CONV_WIDTH) ** -0.5, 0.125, ((0, 4),)),
        "conv_out_weight": centred(key_of[15], (CONV_WIDTH, D), (ATTN_WIDTH + CONV_WIDTH) ** -0.5, 0.125, ((0, 4),)),
    }


NORM_EPSILON = 1e-06

def head_norm(values, head_dim, gain):
    row_count = values.shape[0]
    grouped = values.reshape(row_count, -1, head_dim)
    normed = grouped * lax.rsqrt(lax.optimization_barrier(jnp.mean(grouped * grouped, axis=2, keepdims=True)) + NORM_EPSILON)
    return (normed * gain.reshape(-1, head_dim)).reshape(row_count, -1)

def settle(values):
    return lax.optimization_barrier(values.astype(jnp.bfloat16)).astype(jnp.float32)

def reference(tokens, mix_gain, query_weight, key_weight, value_weight, outer_gate_weight, inner_gate_weight, conv_input_weight, query_gain, key_gain, gate_totals, conv_taps, attn_out_gain, conv_out_gain, attn_out_weight, conv_out_weight):
    widened = tokens.astype(jnp.float32)
    row_scale = lax.rsqrt(lax.optimization_barrier(jnp.sum(widened * widened, axis=1, keepdims=True)) / D + NORM_EPSILON)
    scaled = (widened * mix_gain).astype(jnp.bfloat16)

    def project(weight):
        return row_scale * jnp.dot(scaled, weight, preferred_element_type=jnp.float32)
    queries = settle(head_norm(project(query_weight), HEAD_DIM, query_gain))
    key_rows = settle(head_norm(project(key_weight), HEAD_DIM, key_gain))
    value_rows = settle(project(value_weight))
    query_span = math.gcd(SEQUENCE_TOKENS, 512)
    score_scale = HEAD_DIM ** (-0.5)
    positions = jnp.arange(SEQUENCE_TOKENS, dtype=jnp.int32)

    def one_head(head_index):
        offset = (head_index * HEAD_DIM).astype(jnp.int32)
        head_queries = lax.dynamic_slice_in_dim(queries, offset, HEAD_DIM, 1)
        head_keys = lax.dynamic_slice_in_dim(key_rows, offset, HEAD_DIM, 1)
        head_values = lax.dynamic_slice_in_dim(value_rows, offset, HEAD_DIM, 1)
        head_gates = lax.dynamic_slice_in_dim(gate_totals, head_index.astype(jnp.int32), 1, 1)[:, 0]

        def one_block(block_index):
            start = (block_index * query_span).astype(jnp.int32)
            block_queries = lax.dynamic_slice_in_dim(head_queries, start, query_span, 0)
            block_gates = lax.dynamic_slice_in_dim(head_gates, start, query_span, 0)
            scores = jnp.dot(block_queries, head_keys.T, precision=lax.Precision.HIGHEST) * score_scale
            scores = scores + block_gates[:, None] - head_gates[None, :]
            allowed = positions[None, :] <= (start + jnp.arange(query_span, dtype=jnp.int32))[:, None]
            row_max = lax.optimization_barrier(jnp.max(jnp.where(allowed, scores, -jnp.inf), axis=1, keepdims=True))
            weights = settle(jnp.where(allowed, jnp.exp(scores - row_max), 0.0))
            return jnp.dot(weights, head_values, precision=lax.Precision.HIGHEST)
        blocks = lax.map(one_block, jnp.arange(SEQUENCE_TOKENS // query_span, dtype=jnp.int32))
        return blocks.reshape(SEQUENCE_TOKENS, HEAD_DIM)
    attended = lax.map(one_head, jnp.arange(ATTENTION_HEADS, dtype=jnp.int32))
    attended = jnp.transpose(attended, (1, 0, 2)).reshape(SEQUENCE_TOKENS, ATTN_WIDTH)
    attn_mixed = head_norm(attended, HEAD_DIM, attn_out_gain).astype(jnp.bfloat16)
    gated = settle(project(inner_gate_weight) * project(conv_input_weight))
    padded = jnp.concatenate([jnp.zeros((CONV_K - 1, CONV_WIDTH), jnp.float32), gated], axis=0)
    convolved = conv_taps[0] * padded[0:SEQUENCE_TOKENS]
    for tap_index in range(1, CONV_K):
        convolved = convolved + conv_taps[tap_index] * padded[tap_index:tap_index + SEQUENCE_TOKENS]
    conv_mixed = head_norm(project(outer_gate_weight) * convolved, HEAD_DIM, conv_out_gain).astype(jnp.bfloat16)
    attn_slice = ATTN_WIDTH // N_TP
    conv_slice = CONV_WIDTH // N_TP
    total = jnp.zeros((SEQUENCE_TOKENS, D), jnp.float32)
    for slice_index in range(N_TP):
        attn_lo = slice_index * attn_slice
        conv_lo = slice_index * conv_slice
        partial_value = jnp.dot(attn_mixed[:, attn_lo:attn_lo + attn_slice], attn_out_weight[attn_lo:attn_lo + attn_slice], preferred_element_type=jnp.float32)
        partial_value = partial_value + jnp.dot(conv_mixed[:, conv_lo:conv_lo + conv_slice], conv_out_weight[conv_lo:conv_lo + conv_slice], preferred_element_type=jnp.float32)
        total = total + settle(partial_value)
    return total.astype(jnp.bfloat16)
```

```python
import functools

import jax
import jax.numpy as jnp
from jax import lax
from jax.experimental import pallas as pl
from jax.experimental.pallas import tpu as pltpu
from jax.sharding import PartitionSpec as P

NORM_EPSILON = 1e-06
MESH = pl.DeviceIdType.MESH
CORES = 2
LANES = 128
VMEM = pltpu.VMEM


def head_norm(values, head_dim, gain):
    row_count = values.shape[0]
    grouped = values.reshape(row_count, -1, head_dim)
    normed = grouped * lax.rsqrt(jnp.mean(grouped * grouped, axis=2, keepdims=True) + NORM_EPSILON)
    return (normed * gain.reshape(-1, head_dim)).reshape(row_count, -1)


def greet(devices):
    barrier = pltpu.get_barrier_semaphore()
    for sp, tp in devices:
        pl.semaphore_signal(barrier, inc=1, device_id=(sp, tp), device_id_type=MESH)
    pl.semaphore_wait(barrier, len(devices))


def exchange_kernel(
    sp_count, head_count, block_ref, side_ref, out_ref, side_out, send, side_send, recv, side_recv,
    pass_send, pass_side_send, pass_recv, pass_side_recv, local
):
    sp = lax.axis_index("sp")
    tp = lax.axis_index("tp")
    core = lax.rem(tp, CORES)
    mate = tp + 1 - 2 * core
    targets = sp_count // CORES
    share = targets // head_count
    greet([(lax.rem(sp + step, sp_count), tp) for step in range(1, sp_count)] + [(sp, mate)])
    owner = core == sp // targets

    def copies(slot, head, target):
        return (
            pltpu.make_async_remote_copy(
                block_ref.at[head], out_ref.at[sp], send.at[slot], recv.at[sp],
                device_id=(target, tp), device_id_type=MESH,
            ),
            pltpu.make_async_remote_copy(
                side_ref.at[head], side_out.at[sp], side_send.at[slot], side_recv.at[sp],
                device_id=(target, tp), device_id_type=MESH,
            ),
        )

    def own(head):
        return (
            pltpu.make_async_copy(block_ref.at[head], out_ref.at[sp], local.at[0]),
            pltpu.make_async_copy(side_ref.at[head], side_out.at[sp], local.at[1]),
        )

    def plan(step):
        at = lax.rem(sp + 1 + step, targets)
        return at // share, core * targets + at

    for step in range(targets):
        head, target = plan(step)

        @pl.when(target != sp)
        def _():
            for copy in copies(step, head, target):
                copy.start()

        @pl.when(target == sp)
        def _():
            for copy in own(head):
                copy.start()

    def passed(source):
        return (
            pltpu.make_async_remote_copy(
                out_ref.at[source], out_ref.at[source], pass_send.at[source], pass_recv.at[source],
                device_id=(sp, mate), device_id_type=MESH,
            ),
            pltpu.make_async_remote_copy(
                side_out.at[source], side_out.at[source], pass_side_send.at[source],
                pass_side_recv.at[source], device_id=(sp, mate), device_id_type=MESH,
            ),
        )

    @pl.when(owner)
    def _():
        for step in range(sp_count):
            source = lax.rem(sp + step, sp_count)
            if step == 0:
                for copy in own(0):
                    copy.wait()
            else:
                pltpu.make_async_remote_copy(
                    block_ref.at[0], out_ref.at[source], send.at[0], recv.at[source],
                    device_id=(sp, mate), device_id_type=MESH,
                ).wait_recv()
                pltpu.make_async_remote_copy(
                    side_ref.at[0], side_out.at[source], side_send.at[0], side_recv.at[source],
                    device_id=(sp, mate), device_id_type=MESH,
                ).wait_recv()
            for copy in passed(source):
                copy.start()
        for step in range(sp_count):
            for copy in passed(lax.rem(sp + step, sp_count)):
                copy.wait_send()

    @pl.when(jnp.logical_not(owner))
    def _():
        for step in range(sp_count):
            for copy in passed(lax.rem(sp + step, sp_count)):
                copy.wait_recv()

    for step in range(targets):
        head, target = plan(step)

        @pl.when(target != sp)
        def _():
            for copy in copies(step, head, target):
                copy.wait_send()


def exchange(blocks, sides, sp_count):
    head_count = blocks.shape[0]
    targets = sp_count // CORES
    dma = pltpu.SemaphoreType.DMA
    return pl.pallas_call(
        functools.partial(exchange_kernel, sp_count, head_count),
        out_shape=(
            jax.ShapeDtypeStruct((sp_count,) + blocks.shape[1:], blocks.dtype),
            jax.ShapeDtypeStruct((sp_count,) + sides.shape[1:], sides.dtype),
        ),
        in_specs=[pl.BlockSpec(memory_space=VMEM)] * 2,
        out_specs=(pl.BlockSpec(memory_space=VMEM),) * 2,
        scratch_shapes=[
            dma((targets,)), dma((targets,)), dma((sp_count,)), dma((sp_count,)),
            dma((sp_count,)), dma((sp_count,)), dma((sp_count,)), dma((sp_count,)), dma((2,)),
        ],
        compiler_params=pltpu.CompilerParams(
            collective_id=0, has_side_effects=True, vmem_limit_bytes=48 * 1024 * 1024
        ),
    )(blocks, sides)


def giveback_kernel(sp_count, head_count, block_ref, out_ref, send, recv, local):
    sp = lax.axis_index("sp")
    tp = lax.axis_index("tp")
    core = lax.rem(tp, CORES)
    first = tp - core
    targets = sp_count // CORES
    greet(
        [
            (lax.rem(sp + step, sp_count), first + lax.rem(core + other, CORES))
            for step in range(sp_count)
            for other in range(CORES)
            if step or other
        ]
    )
    home = sp // targets
    slot = lax.rem(sp, targets) * CORES + core
    home_here = home == core
    for step in range(1, sp_count + 1):
        source = lax.rem(sp + step, sp_count)
        away = pltpu.make_async_remote_copy(
            block_ref.at[source], out_ref.at[slot], send.at[step - 1], recv.at[slot],
            device_id=(source, first + home), device_id_type=MESH,
        )
        if step < sp_count:
            away.start()
        else:

            @pl.when(home_here)
            def _():
                pltpu.make_async_copy(block_ref.at[source], out_ref.at[slot], local).start()

            @pl.when(jnp.logical_not(home_here))
            def _():
                away.start()

    for index in range(targets * CORES):
        giver = core * targets + index // CORES
        here = jnp.logical_and(giver == sp, core == index % CORES)

        @pl.when(here)
        def _():
            pltpu.make_async_copy(block_ref.at[0], out_ref.at[index], local).wait()

        @pl.when(jnp.logical_not(here))
        def _():
            pltpu.make_async_remote_copy(
                block_ref.at[0], out_ref.at[index], send.at[0], recv.at[index],
                device_id=(sp, tp + 1 - 2 * core), device_id_type=MESH,
            ).wait_recv()

    for step in range(1, sp_count + 1):
        source = lax.rem(sp + step, sp_count)
        away = pltpu.make_async_remote_copy(
            block_ref.at[source], out_ref.at[slot], send.at[step - 1], recv.at[slot],
            device_id=(source, first + home), device_id_type=MESH,
        )
        if step < sp_count:
            away.wait_send()
        else:

            @pl.when(jnp.logical_not(home_here))
            def _():
                away.wait_send()


def giveback(blocks, head_count):
    sp_count = blocks.shape[0]
    dma = pltpu.SemaphoreType.DMA
    return pl.pallas_call(
        functools.partial(giveback_kernel, sp_count, head_count),
        out_shape=jax.ShapeDtypeStruct((sp_count,) + blocks.shape[1:], blocks.dtype),
        in_specs=[pl.BlockSpec(memory_space=VMEM)],
        out_specs=pl.BlockSpec(memory_space=VMEM),
        scratch_shapes=[dma((sp_count,)), dma((sp_count,)), dma],
        compiler_params=pltpu.CompilerParams(
            collective_id=1, has_side_effects=True, vmem_limit_bytes=32 * 1024 * 1024
        ),
    )(blocks)


def attention_kernel(count_ref, query_ref, key_ref, kv_ref, gain_ref, out_ref):
    rows = query_ref.shape[1]
    width = gain_ref.shape[1]
    full = count_ref[pl.program_id(0)]
    queries = query_ref[0]

    def fold(index, carried, masked):
        top, total = carried
        at = pl.ds(pl.multiple_of(index * rows, rows), rows)
        scores = lax.dot_general(
            queries, key_ref[at, :], (((1,), (1,)), ((), ())), preferred_element_type=jnp.float32
        )
        if masked:
            row = lax.broadcasted_iota(jnp.int32, scores.shape, 0)
            column = lax.broadcasted_iota(jnp.int32, scores.shape, 1)
            scores = jnp.where(column <= row, scores, -jnp.inf)
        new_top = jnp.maximum(top, jnp.max(scores, axis=1, keepdims=True))
        weights = jnp.exp(scores - new_top).astype(jnp.bfloat16)
        added = jnp.dot(weights, kv_ref[at, :], preferred_element_type=jnp.float32)
        return new_top, total * jnp.exp(top - new_top) + added

    carried = (
        jnp.full((rows, 1), -1e30, jnp.float32),
        jnp.zeros((rows, kv_ref.shape[1]), jnp.float32),
    )
    carried = lax.fori_loop(0, full, lambda index, now: fold(index, now, False), carried)
    _, total = fold(full, carried, True)
    attended = total[:, width:]
    scale = lax.rsqrt(jnp.mean(attended * attended, axis=1, keepdims=True) + NORM_EPSILON)
    mixed = (attended * scale * gain_ref[...]).astype(jnp.bfloat16)
    out_ref[0] = jnp.concatenate([mixed[: rows // 2], mixed[rows // 2 :]], axis=1)


def attention(counts, queries, keys, kv, gain):
    sp_count, rows, _ = queries.shape
    return pl.pallas_call(
        attention_kernel,
        grid_spec=pltpu.PrefetchScalarGridSpec(
            num_scalar_prefetch=1,
            grid=(sp_count,),
            in_specs=[
                pl.BlockSpec((1, rows, queries.shape[2]), lambda i, n: (i, 0, 0)),
                pl.BlockSpec(keys.shape, lambda i, n: (0, 0)),
                pl.BlockSpec(kv.shape, lambda i, n: (0, 0)),
                pl.BlockSpec(gain.shape, lambda i, n: (0, 0)),
            ],
            out_specs=pl.BlockSpec((1, rows // 2, LANES), lambda i, n: (i, 0, 0)),
        ),
        out_shape=jax.ShapeDtypeStruct((sp_count, rows // 2, LANES), jnp.bfloat16),
        compiler_params=pltpu.CompilerParams(vmem_limit_bytes=48 * 1024 * 1024),
    )(counts, queries, keys, kv, gain)


def split_three(values):
    high = lax.reduce_precision(values, 8, 7)
    rest = values - high
    middle = lax.reduce_precision(rest, 8, 7)
    low = rest - middle
    return [part.astype(jnp.bfloat16) for part in (high, middle, low)]


def shifted(shard, axis, by):
    devices = lax.axis_size(axis)
    pairs = [(i, i + by) for i in range(devices) if 0 <= i + by < devices]
    return lax.ppermute(shard, axis, pairs)


def attend(queries, key_rows, value_rows, gate_totals, attn_out_gain, head_dim):
    rows, width = queries.shape
    heads = width // head_dim
    sp = lax.axis_index("sp")
    sp_count = lax.axis_size("sp")
    core = lax.rem(lax.axis_index("tp"), CORES)
    targets = sp_count // CORES
    share = targets // heads
    pieces = CORES * share
    piece = rows // pieces
    by_head = lambda array: array.reshape(rows, heads, head_dim).transpose(1, 0, 2)
    kv = jnp.concatenate([by_head(key_rows), by_head(value_rows)], axis=2)
    head_queries = by_head(queries)
    packed = jnp.concatenate([head_queries[:, : rows // 2], head_queries[:, rows // 2 :]], axis=2)
    blocks = jnp.concatenate([kv, packed], axis=1)
    gate_rows = gate_totals.T.reshape(heads, rows // LANES, LANES)
    gain_rows = jnp.pad(attn_out_gain.reshape(heads, 1, head_dim), ((0, 0), (0, 7), (0, LANES - head_dim)))
    sides = jnp.concatenate([gate_rows, gain_rows], axis=1)

    blocks, sides = exchange(blocks, sides, sp_count)

    gates = sides[:, : rows // LANES].reshape(sp_count * rows)
    gain = sides[0, rows // LANES : rows // LANES + 1, :head_dim]
    kv = blocks[:, :rows].reshape(sp_count * rows, 2 * head_dim)
    packed = blocks[:, rows:]
    unpacked = jnp.concatenate([packed[:, :, :head_dim], packed[:, :, head_dim:]], axis=1)
    place = lax.rem(sp, share) * CORES + core

    def pick(array):
        pairs = array.reshape((sp_count // 2, 2, pieces, piece) + array.shape[2:])
        even = lax.dynamic_index_in_dim(pairs[:, 0], place, 1, False)
        odd = lax.dynamic_index_in_dim(pairs[:, 1], pieces - 1 - place, 1, False)
        return jnp.stack([even, odd], axis=1).reshape((sp_count, piece) + array.shape[2:])

    mine = pick(unpacked)
    mine_gates = pick(gates.reshape(sp_count, rows))
    one = lambda array: jnp.ones(array.shape, jnp.bfloat16)
    extra = split_three(mine_gates)
    spare = 2 * head_dim - head_dim - 6
    query_side = jnp.concatenate(
        [(mine.astype(jnp.float32) * head_dim ** (-0.5)).astype(jnp.bfloat16)]
        + [jnp.stack(extra + [one(mine_gates)] * 3, axis=2)]
        + [jnp.zeros(mine_gates.shape + (spare,), jnp.bfloat16)],
        axis=2,
    )
    extra = split_three(-gates)
    key_side = jnp.concatenate(
        [kv[:, :head_dim], jnp.stack([one(gates)] * 3 + extra, axis=1)]
        + [jnp.zeros(gates.shape + (spare,), jnp.bfloat16)],
        axis=1,
    )
    source = jnp.arange(sp_count, dtype=jnp.int32)
    counts = source * pieces + jnp.where(source % 2 == 0, place, pieces - 1 - place)
    finished = attention(counts.astype(jnp.int32), query_side, key_side, kv, gain)

    back = giveback(finished, heads)
    back = back.reshape(heads, pieces, piece // 2, 2, head_dim)
    back = jnp.where(sp % 2 == 0, back, back[:, ::-1])
    return back.transpose(1, 3, 2, 0, 4).reshape(rows, width)


def per_device(
    tokens,
    mix_gain,
    query_weight,
    key_weight,
    value_weight,
    outer_gate_weight,
    inner_gate_weight,
    conv_input_weight,
    query_gain,
    key_gain,
    gate_totals,
    conv_taps,
    attn_out_gain,
    conv_out_gain,
    attn_out_weight,
    conv_out_weight,
):
    row_count = tokens.shape[0]
    head_dim = query_gain.shape[0]
    gathered = lax.all_gather(tokens, "tp", axis=1, tiled=True).astype(jnp.float32)
    squares = jnp.sum(gathered * gathered, axis=1)
    scaled = (gathered * mix_gain).astype(jnp.bfloat16)
    row_scale = lax.rsqrt(squares / mix_gain.shape[0] + NORM_EPSILON)[:, None]

    def project(weight):
        return jnp.dot(scaled, weight, preferred_element_type=jnp.float32) * row_scale

    queries = head_norm(project(query_weight), head_dim, query_gain).astype(jnp.bfloat16)
    key_rows = head_norm(project(key_weight), head_dim, key_gain).astype(jnp.bfloat16)
    value_rows = project(value_weight).astype(jnp.bfloat16)
    proj_outer = project(outer_gate_weight)
    gated = (project(inner_gate_weight) * project(conv_input_weight)).astype(jnp.bfloat16)
    attn_mixed = attend(queries, key_rows, value_rows, gate_totals, attn_out_gain, head_dim)
    tap_count = conv_taps.shape[0]
    prior_rows = shifted(gated[row_count - tap_count + 1 :], "sp", 1)
    padded = jnp.concatenate([prior_rows, gated], axis=0).astype(jnp.float32)
    convolved = conv_taps[0] * padded[0:row_count]
    for tap_index in range(1, tap_count):
        convolved = convolved + conv_taps[tap_index] * padded[tap_index : tap_index + row_count]
    conv_mixed = head_norm(proj_outer * convolved, head_dim, conv_out_gain).astype(jnp.bfloat16)
    partial = jnp.dot(attn_mixed, attn_out_weight, preferred_element_type=jnp.float32)
    partial = partial + jnp.dot(conv_mixed, conv_out_weight, preferred_element_type=jnp.float32)
    return lax.psum_scatter(partial.astype(jnp.bfloat16), "tp", scatter_dimension=0, tiled=True)


def solution(mesh):
    placed = (
        P("sp", "tp"),
        P(),
        P(None, "tp"),
        P(None, "tp"),
        P(None, "tp"),
        P(None, "tp"),
        P(None, "tp"),
        P(None, "tp"),
        P(),
        P(),
        P("sp", "tp"),
        P(None, "tp"),
        P("tp"),
        P("tp"),
        P("tp", None),
        P("tp", None),
    )
    return jax.shard_map(
        per_device, mesh=mesh, in_specs=placed, out_specs=P(("sp", "tp"), None), check_vma=False
    )
```

```python
import functools

import jax
import jax.numpy as jnp
from jax import lax
from jax.experimental import pallas as pl
from jax.experimental.pallas import tpu as pltpu
from jax.sharding import PartitionSpec as P

NORM_EPSILON = 1e-06
MESH = pl.DeviceIdType.MESH
CORES = 2
LANES = 128
VMEM = pltpu.VMEM


def greet(devices):
    barrier = pltpu.get_barrier_semaphore()
    for sp, tp in devices:
        pl.semaphore_signal(barrier, inc=1, device_id=(sp, tp), device_id_type=MESH)
    pl.semaphore_wait(barrier, len(devices))


def mesh_copy(src, dst, send, recv, device):
    return pltpu.make_async_remote_copy(
        src, dst, send, recv, device_id=device, device_id_type=MESH
    )


def front_kernel(
    plan, tokens_ref, mix_ref, qkv_gain_ref, taps_ref, conv_gain_ref, side_ref, *refs
):
    sp_count, tp_count, head_count, head_dim, chunk = plan
    weight_refs = refs[:6]
    kv_out, query_out, side_out, conv_out = refs[6:10]
    (
        weights, gathered, scaled, kv_send, query_send, outer, padded, edge_send, edge_recv,
        weight_sem, own_sem, cross_send, mate_send, tok_pass_send, tok_recv,
        kv_ssem, kv_rsem, query_ssem, query_rsem, side_ssem, side_rsem,
        kv_psem, kv_prsem, query_psem, query_prsem, side_psem, side_prsem, local, edge_sem,
    ) = refs[10:]
    sp = lax.axis_index("sp")
    tp = lax.axis_index("tp")
    core = lax.rem(tp, CORES)
    mate = tp + 1 - 2 * core
    chips = tp_count // CORES
    targets = sp_count // CORES
    share = targets // head_count
    rows, features = tokens_ref.shape
    chunks = rows // chunk
    half = chunk // 2
    width = head_count * head_dim
    order = [chunks - 1] + list(range(chunks - 1))

    loads = [
        pltpu.make_async_copy(ref, weights.at[index], weight_sem.at[index])
        for index, ref in enumerate(weight_refs)
    ]
    for load in loads:
        load.start()
    mine = pltpu.make_async_copy(tokens_ref, gathered.at[tp], own_sem)
    mine.start()
    padded[0:8, :] = jnp.zeros((8, width), jnp.float32)
    greet(
        [(lax.rem(sp + step, sp_count), tp) for step in range(1, sp_count)]
        + [(sp, mate)]
        + [(sp, lax.rem(tp + CORES * step, tp_count)) for step in range(1, chips)]
    )

    def block(number):
        return pl.ds(number * chunk, chunk)

    def to_mate(number):
        return mesh_copy(
            tokens_ref.at[block(number)], gathered.at[tp, block(number)], mate_send.at[number],
            tok_recv.at[tp, number], (sp, mate),
        )

    def across(step, number):
        return mesh_copy(
            tokens_ref.at[block(number)], gathered.at[tp, block(number)],
            cross_send.at[step - 1, number], tok_recv.at[tp, number],
            (sp, lax.rem(tp + CORES * step, tp_count)),
        )

    def token_pass(step, number):
        other = lax.rem(tp + CORES * step, tp_count)
        return mesh_copy(
            gathered.at[other, block(number)], gathered.at[other, block(number)],
            tok_pass_send.at[step - 1, number], tok_recv.at[other, number], (sp, mate),
        )

    def token_arrival(source, number):
        return mesh_copy(
            tokens_ref.at[block(number)], gathered.at[source, block(number)], mate_send.at[number],
            tok_recv.at[source, number], (sp, mate),
        )

    for number in order:
        for step in range(1, chips):
            across(step, number).start()
        to_mate(number).start()

    owner = core == sp // targets

    def target_of(step):
        at = lax.rem(sp + 1 + step, targets)
        return at // share, core * targets + at

    def side_copy(step, head, target):
        return mesh_copy(
            side_ref.at[head], side_out.at[sp], side_ssem.at[step], side_rsem.at[sp], (target, tp)
        )

    def kv_copy(step, number, head, target):
        return mesh_copy(
            kv_send.at[head, block(number)], kv_out.at[sp, block(number)],
            kv_ssem.at[step, number], kv_rsem.at[sp, number], (target, tp),
        )

    def query_copy(step, number, head, target):
        at = pl.ds(number * half, half)
        return mesh_copy(
            query_send.at[head, at], query_out.at[sp, at],
            query_ssem.at[step, number], query_rsem.at[sp, number], (target, tp),
        )

    def kept(number, head):
        at = pl.ds(number * half, half)
        return (
            pltpu.make_async_copy(
                kv_send.at[head, block(number)], kv_out.at[sp, block(number)], local.at[0, number]
            ),
            pltpu.make_async_copy(
                query_send.at[head, at], query_out.at[sp, at], local.at[1, number]
            ),
        )

    def kept_side(head):
        return pltpu.make_async_copy(side_ref.at[head], side_out.at[sp], local.at[2, 0])

    for step in range(targets):
        head, target = target_of(step)

        @pl.when(target != sp)
        def _():
            side_copy(step, head, target).start()

        @pl.when(target == sp)
        def _():
            kept_side(head).start()

    ones_row = lax.broadcasted_iota(jnp.int32, (width, width), 0) // head_dim
    ones_column = lax.broadcasted_iota(jnp.int32, (width, width), 1) // head_dim
    spread = jnp.where(ones_row == ones_column, 1.0 / head_dim, 0.0).astype(jnp.bfloat16)

    def normed(values, gain):
        squares = values * values
        high = squares.astype(jnp.bfloat16)
        low = (squares - high.astype(jnp.float32)).astype(jnp.bfloat16)
        mean = jnp.dot(high, spread, preferred_element_type=jnp.float32)
        mean = mean + jnp.dot(low, spread, preferred_element_type=jnp.float32)
        return values * lax.rsqrt(mean + NORM_EPSILON) * gain

    mine.wait()
    for load in loads:
        load.wait()
    for number in order:
        here = block(number)
        for step in range(1, chips):
            token_arrival(lax.rem(tp + CORES * step, tp_count), number).wait_recv()
            token_pass(step, number).start()
        token_arrival(mate, number).wait_recv()
        for step in range(1, chips):
            token_arrival(lax.rem(mate + CORES * step, tp_count), number).wait_recv()
        total = jnp.zeros((chunk, 1), jnp.float32)
        for source in range(tp_count):
            part = gathered[source, here, :].astype(jnp.float32)
            at = slice(source * features, (source + 1) * features)
            total = total + jnp.sum(part * part, axis=1, keepdims=True)
            scaled[:, at] = (part * mix_ref[:, at]).astype(jnp.bfloat16)
        row_scale = lax.rsqrt(total / (tp_count * features) + NORM_EPSILON)

        def project(index):
            product = jnp.dot(scaled[...], weights[index], preferred_element_type=jnp.float32)
            return product * row_scale

        keys = normed(project(1), qkv_gain_ref[1:2, :]).astype(jnp.bfloat16)
        values = project(2).astype(jnp.bfloat16)
        queries = normed(project(0), qkv_gain_ref[0:1, :]).astype(jnp.bfloat16)
        queries = (queries.astype(jnp.float32) * head_dim ** (-0.5)).astype(jnp.bfloat16)
        for head in range(head_count):
            at = slice(head * head_dim, (head + 1) * head_dim)
            kv_send[head, here, :] = jnp.concatenate([keys[:, at], values[:, at]], axis=1)
            query_send[head, pl.ds(number * half, half), :] = jnp.concatenate(
                [queries[:half, at], queries[half:, at]], axis=1
            )
        for step in range(targets):
            head, target = target_of(step)

            @pl.when(target != sp)
            def _():
                kv_copy(step, number, head, target).start()
                query_copy(step, number, head, target).start()

            @pl.when(target == sp)
            def _():
                for copy in kept(number, head):
                    copy.start()

        outer[here, :] = project(3)
        gated = (project(4) * project(5)).astype(jnp.bfloat16)
        padded[pl.ds(8 + number * chunk, chunk), :] = gated.astype(jnp.float32)
        if number == chunks - 1:
            edge_send[...] = gated[chunk - 16 :, :]

            @pl.when(sp < sp_count - 1)
            def _():
                mesh_copy(
                    edge_send, edge_recv, edge_sem.at[0], edge_sem.at[1],
                    (lax.rem(sp + 1, sp_count), tp),
                ).start()

    edge = mesh_copy(
        edge_send, edge_recv, edge_sem.at[0], edge_sem.at[1], (lax.rem(sp + 1, sp_count), tp)
    )

    @pl.when(sp > 0)
    def _():
        edge.wait_recv()
        padded[0:8, :] = edge_recv[8:16, :].astype(jnp.float32)

    taps = taps_ref.shape[0]
    for number in range(chunks):
        convolved = jnp.zeros((chunk, width), jnp.float32)
        for tap in range(taps):
            at = pl.ds(8 - taps + 1 + tap + number * chunk, chunk)
            convolved = convolved + taps_ref[tap : tap + 1, :] * padded[at, :]
        conv_out[block(number), :] = normed(
            outer[block(number), :] * convolved, conv_gain_ref[...]
        ).astype(jnp.bfloat16)

    def kv_pass(source, number):
        return mesh_copy(
            kv_out.at[source, block(number)], kv_out.at[source, block(number)],
            kv_psem.at[source, number], kv_prsem.at[source, number], (sp, mate),
        )

    def query_pass(source, number):
        at = pl.ds(number * half, half)
        return mesh_copy(
            query_out.at[source, at], query_out.at[source, at],
            query_psem.at[source, number], query_prsem.at[source, number], (sp, mate),
        )

    def side_pass(source):
        return mesh_copy(
            side_out.at[source], side_out.at[source], side_psem.at[source], side_prsem.at[source],
            (sp, mate),
        )

    sources = [lax.rem(sp + step, sp_count) for step in range(sp_count)]

    @pl.when(owner)
    def _():
        for step, source in enumerate(sources):
            if step == 0:
                kept_side(0).wait()
            else:
                mesh_copy(
                    side_ref.at[0], side_out.at[source], side_ssem.at[0], side_rsem.at[source],
                    (sp, mate),
                ).wait_recv()
            side_pass(source).start()
        for number in order:
            at = pl.ds(number * half, half)
            for step, source in enumerate(sources):
                if step == 0:
                    for copy in kept(number, 0):
                        copy.wait()
                else:
                    mesh_copy(
                        kv_send.at[0, block(number)], kv_out.at[source, block(number)],
                        kv_ssem.at[0, number], kv_rsem.at[source, number], (sp, mate),
                    ).wait_recv()
                    mesh_copy(
                        query_send.at[0, at], query_out.at[source, at],
                        query_ssem.at[0, number], query_rsem.at[source, number], (sp, mate),
                    ).wait_recv()
                kv_pass(source, number).start()
                query_pass(source, number).start()
        for source in sources:
            side_pass(source).wait_send()
            for number in order:
                kv_pass(source, number).wait_send()
                query_pass(source, number).wait_send()

    @pl.when(jnp.logical_not(owner))
    def _():
        for source in sources:
            side_pass(source).wait_recv()
            for number in order:
                kv_pass(source, number).wait_recv()
                query_pass(source, number).wait_recv()

    for step in range(targets):
        head, target = target_of(step)

        @pl.when(target != sp)
        def _():
            side_copy(step, head, target).wait_send()
            for number in order:
                kv_copy(step, number, head, target).wait_send()
                query_copy(step, number, head, target).wait_send()

    for number in order:
        to_mate(number).wait_send()
        for step in range(1, chips):
            across(step, number).wait_send()
            token_pass(step, number).wait_send()

    @pl.when(sp < sp_count - 1)
    def _():
        edge.wait_send()


def front(tokens, mix_gain, qkv_gain, taps, conv_gain, sides, weights, head_dim, piece):
    sp_count = lax.axis_size("sp")
    tp_count = lax.axis_size("tp")
    rows, features = tokens.shape
    width = weights[0].shape[1]
    heads = width // head_dim
    chunk = min(256, piece)
    chunks = rows // chunk
    chips = tp_count // CORES
    targets = sp_count // CORES
    bf16 = jnp.bfloat16
    dma = pltpu.SemaphoreType.DMA
    across = (max(chips - 1, 1), chunks)
    vmem = pl.BlockSpec(memory_space=VMEM)
    return pl.pallas_call(
        functools.partial(front_kernel, (sp_count, tp_count, heads, head_dim, chunk)),
        out_shape=(
            jax.ShapeDtypeStruct((sp_count, rows, LANES), bf16),
            jax.ShapeDtypeStruct((sp_count, rows // 2, LANES), bf16),
            jax.ShapeDtypeStruct((sp_count,) + sides.shape[1:], sides.dtype),
            jax.ShapeDtypeStruct((rows, width), bf16),
        ),
        in_specs=[vmem] * 6 + [pl.BlockSpec(memory_space=pl.ANY)] * 6,
        out_specs=(vmem,) * 4,
        scratch_shapes=[
            VMEM((6,) + weights[0].shape, bf16),
            VMEM((tp_count, rows, features), bf16),
            VMEM((chunk, tp_count * features), bf16),
            VMEM((heads, rows, LANES), bf16),
            VMEM((heads, rows // 2, LANES), bf16),
            VMEM((rows, width), jnp.float32),
            VMEM((rows + 8, width), jnp.float32),
            VMEM((16, width), bf16),
            VMEM((16, width), bf16),
            dma((6,)), dma, dma(across), dma((chunks,)), dma(across), dma((tp_count, chunks)),
            dma((targets, chunks)), dma((sp_count, chunks)),
            dma((targets, chunks)), dma((sp_count, chunks)),
            dma((targets,)), dma((sp_count,)),
            dma((sp_count, chunks)), dma((sp_count, chunks)),
            dma((sp_count, chunks)), dma((sp_count, chunks)),
            dma((sp_count,)), dma((sp_count,)),
            dma((3, chunks)), dma((2,)),
        ],
        compiler_params=pltpu.CompilerParams(
            collective_id=0, has_side_effects=True, vmem_limit_bytes=56 * 1024 * 1024
        ),
    )(tokens, mix_gain, qkv_gain, taps, conv_gain, sides, *weights)


def giveback_kernel(sp_count, head_count, block_ref, out_ref, send, recv, local):
    sp = lax.axis_index("sp")
    tp = lax.axis_index("tp")
    core = lax.rem(tp, CORES)
    first = tp - core
    targets = sp_count // CORES
    greet(
        [
            (lax.rem(sp + step, sp_count), first + lax.rem(core + other, CORES))
            for step in range(sp_count)
            for other in range(CORES)
            if step or other
        ]
    )
    home = sp // targets
    slot = lax.rem(sp, targets) * CORES + core
    home_here = home == core
    for step in range(1, sp_count + 1):
        source = lax.rem(sp + step, sp_count)
        away = pltpu.make_async_remote_copy(
            block_ref.at[source], out_ref.at[slot], send.at[step - 1], recv.at[slot],
            device_id=(source, first + home), device_id_type=MESH,
        )
        if step < sp_count:
            away.start()
        else:

            @pl.when(home_here)
            def _():
                pltpu.make_async_copy(block_ref.at[source], out_ref.at[slot], local).start()

            @pl.when(jnp.logical_not(home_here))
            def _():
                away.start()

    for index in range(targets * CORES):
        giver = core * targets + index // CORES
        here = jnp.logical_and(giver == sp, core == index % CORES)

        @pl.when(here)
        def _():
            pltpu.make_async_copy(block_ref.at[0], out_ref.at[index], local).wait()

        @pl.when(jnp.logical_not(here))
        def _():
            pltpu.make_async_remote_copy(
                block_ref.at[0], out_ref.at[index], send.at[0], recv.at[index],
                device_id=(sp, tp + 1 - 2 * core), device_id_type=MESH,
            ).wait_recv()

    for step in range(1, sp_count + 1):
        source = lax.rem(sp + step, sp_count)
        away = pltpu.make_async_remote_copy(
            block_ref.at[source], out_ref.at[slot], send.at[step - 1], recv.at[slot],
            device_id=(source, first + home), device_id_type=MESH,
        )
        if step < sp_count:
            away.wait_send()
        else:

            @pl.when(jnp.logical_not(home_here))
            def _():
                away.wait_send()


def giveback(blocks, head_count):
    sp_count = blocks.shape[0]
    dma = pltpu.SemaphoreType.DMA
    return pl.pallas_call(
        functools.partial(giveback_kernel, sp_count, head_count),
        out_shape=jax.ShapeDtypeStruct((sp_count,) + blocks.shape[1:], blocks.dtype),
        in_specs=[pl.BlockSpec(memory_space=VMEM)],
        out_specs=pl.BlockSpec(memory_space=VMEM),
        scratch_shapes=[dma((sp_count,)), dma((sp_count,)), dma],
        compiler_params=pltpu.CompilerParams(
            collective_id=1, has_side_effects=True, vmem_limit_bytes=32 * 1024 * 1024
        ),
    )(blocks)


def attention_kernel(count_ref, query_ref, kv_ref, side_ref, out_ref):
    piece_rows = out_ref.shape[1] * 2
    head_dim = LANES // 2
    chunk_half = min(128, piece_rows // 2)
    full = count_ref[0, pl.program_id(0)]
    begin = pl.multiple_of(count_ref[1, pl.program_id(0)], chunk_half)
    side_rows = piece_rows // LANES
    rows = kv_ref.shape[1]
    per_source = rows // piece_rows
    low = lax.broadcasted_iota(jnp.int32, (chunk_half, LANES), 1) < head_dim
    tiles = []
    for number in range(piece_rows // (2 * chunk_half)):
        pair = query_ref[0, pl.ds(begin + number * chunk_half, chunk_half), :].astype(jnp.float32)
        left = jnp.where(low, pair, 0.0)
        right = jnp.where(low, pltpu.roll(pair, head_dim, 1), 0.0)
        tiles.append(jnp.concatenate([left, right], axis=0).astype(jnp.bfloat16))
    tile_rows = 2 * chunk_half

    def fold(index, carried, masked):
        source = index // per_source
        part = lax.rem(index, per_source)
        kv = kv_ref[source, pl.ds(pl.multiple_of(part * piece_rows, piece_rows), piece_rows), :]
        gates = side_ref[source, pl.ds(part * side_rows, side_rows), :]
        gate_row = jnp.concatenate([gates[row : row + 1, :] for row in range(side_rows)], axis=1)
        results = []
        for number, (top, total) in enumerate(carried):
            scores = lax.dot_general(
                tiles[number], kv, (((1,), (1,)), ((), ())), preferred_element_type=jnp.float32
            ) - gate_row
            if masked:
                row = lax.broadcasted_iota(jnp.int32, scores.shape, 0) + number * tile_rows
                column = lax.broadcasted_iota(jnp.int32, scores.shape, 1)
                scores = jnp.where(column <= row, scores, -jnp.inf)
            new_top = jnp.maximum(top, jnp.max(scores, axis=1, keepdims=True))
            weights = jnp.exp(scores - new_top).astype(jnp.bfloat16)
            added = jnp.dot(weights, kv, preferred_element_type=jnp.float32)
            results.append((new_top, total * jnp.exp(top - new_top) + added))
        return tuple(results)

    carried = tuple(
        (
            jnp.full((tile_rows, 1), -1e30, jnp.float32),
            jnp.zeros((tile_rows, LANES), jnp.float32),
        )
        for _ in tiles
    )
    carried = lax.fori_loop(0, full, lambda index, now: fold(index, now, False), carried)
    carried = fold(full, carried, True)
    gain = side_ref[0, rows // LANES : rows // LANES + 1, :head_dim]
    mixed = []
    for _, total in carried:
        attended = total[:, head_dim:]
        scale = lax.rsqrt(jnp.mean(attended * attended, axis=1, keepdims=True) + NORM_EPSILON)
        mixed.append((attended * scale * gain).astype(jnp.bfloat16))
    mixed = jnp.concatenate(mixed, axis=0)
    half = piece_rows // 2
    out_ref[0] = jnp.concatenate([mixed[:half], mixed[half:]], axis=1)


def attention(counts, queries, kv, sides, piece):
    sp_count = queries.shape[0]
    return pl.pallas_call(
        attention_kernel,
        grid_spec=pltpu.PrefetchScalarGridSpec(
            num_scalar_prefetch=1,
            grid=(sp_count,),
            in_specs=[
                pl.BlockSpec((1,) + queries.shape[1:], lambda i, n: (i, 0, 0)),
                pl.BlockSpec(kv.shape, lambda i, n: (0, 0, 0)),
                pl.BlockSpec(sides.shape, lambda i, n: (0, 0, 0)),
            ],
            out_specs=pl.BlockSpec((1, piece // 2, LANES), lambda i, n: (i, 0, 0)),
        ),
        out_shape=jax.ShapeDtypeStruct((sp_count, piece // 2, LANES), jnp.bfloat16),
        compiler_params=pltpu.CompilerParams(vmem_limit_bytes=48 * 1024 * 1024),
    )(counts, queries, kv, sides)


def per_device(
    tokens,
    mix_gain,
    query_weight,
    key_weight,
    value_weight,
    outer_gate_weight,
    inner_gate_weight,
    conv_input_weight,
    query_gain,
    key_gain,
    gate_totals,
    conv_taps,
    attn_out_gain,
    conv_out_gain,
    attn_out_weight,
    conv_out_weight,
):
    rows = tokens.shape[0]
    head_dim = query_gain.shape[0]
    width = query_weight.shape[1]
    heads = width // head_dim
    sp = lax.axis_index("sp")
    sp_count = lax.axis_size("sp")
    core = lax.rem(lax.axis_index("tp"), CORES)
    share = sp_count // CORES // heads
    pieces = CORES * share
    piece = rows // pieces
    gate_rows = gate_totals.T.reshape(heads, rows // LANES, LANES)
    gain_rows = jnp.pad(
        attn_out_gain.reshape(heads, 1, head_dim), ((0, 0), (0, 7), (0, LANES - head_dim))
    )
    sides = jnp.concatenate([gate_rows, gain_rows], axis=1)
    qkv_gain = jnp.stack([jnp.tile(query_gain, heads), jnp.tile(key_gain, heads)])
    kv, queries, sides, conv_mixed = front(
        tokens,
        mix_gain.reshape(1, -1),
        qkv_gain,
        conv_taps,
        conv_out_gain.reshape(1, -1),
        sides,
        (
            query_weight,
            key_weight,
            value_weight,
            outer_gate_weight,
            inner_gate_weight,
            conv_input_weight,
        ),
        head_dim,
        piece,
    )
    place = lax.rem(sp, share) * CORES + core
    source = jnp.arange(sp_count, dtype=jnp.int32)
    spot = jnp.where(source % 2 == 0, place, pieces - 1 - place)
    counts = jnp.stack([source * pieces + spot, spot * (piece // 2)]).astype(jnp.int32)
    finished = attention(counts, queries, kv, sides, piece)
    back = giveback(finished, heads)
    back = back.reshape(heads, pieces, piece // 2, 2, head_dim)
    back = jnp.where(sp % 2 == 0, back, back[:, ::-1])
    attn_mixed = back.transpose(1, 3, 2, 0, 4).reshape(rows, width)
    partial = jnp.dot(attn_mixed, attn_out_weight, preferred_element_type=jnp.float32)
    partial = partial + jnp.dot(conv_mixed, conv_out_weight, preferred_element_type=jnp.float32)
    return lax.psum_scatter(partial.astype(jnp.bfloat16), "tp", scatter_dimension=0, tiled=True)


def solution(mesh):
    placed = (
        P("sp", "tp"),
        P(),
        P(None, "tp"),
        P(None, "tp"),
        P(None, "tp"),
        P(None, "tp"),
        P(None, "tp"),
        P(None, "tp"),
        P(),
        P(),
        P("sp", "tp"),
        P(None, "tp"),
        P("tp"),
        P("tp"),
        P("tp", None),
        P("tp", None),
    )
    return jax.shard_map(
        per_device, mesh=mesh, in_specs=placed, out_specs=P(("sp", "tp"), None), check_vma=False
    )
```

```python
import functools

import jax
import jax.numpy as jnp
from jax import lax
from jax.experimental import pallas as pl
from jax.experimental.pallas import tpu as pltpu
from jax.sharding import PartitionSpec as P

NORM_EPSILON = 1e-06
MESH = pl.DeviceIdType.MESH
CORES = 2
LANES = 128
VMEM = pltpu.VMEM


def greet(devices):
    barrier = pltpu.get_barrier_semaphore()
    for sp, tp in devices:
        pl.semaphore_signal(barrier, inc=1, device_id=(sp, tp), device_id_type=MESH)
    pl.semaphore_wait(barrier, len(devices))


def mesh_copy(src, dst, send, recv, device):
    return pltpu.make_async_remote_copy(
        src, dst, send, recv, device_id=device, device_id_type=MESH
    )


def front_kernel(
    plan, tokens_ref, mix_ref, qkv_gain_ref, taps_ref, conv_gain_ref, side_ref, *refs
):
    sp_count, tp_count, head_count, head_dim, chunk = plan
    weight_refs = refs[:6]
    kv_out, query_out, side_out, conv_out = refs[6:10]
    (
        weights, gathered, scaled, kv_send, query_send, outer, padded, edge_send, edge_recv,
        weight_sem, own_sem, cross_send, mate_send, tok_pass_send, tok_recv,
        kv_ssem, kv_rsem, query_ssem, query_rsem, side_ssem, side_rsem,
        kv_psem, kv_prsem, query_psem, query_prsem, side_psem, side_prsem, local, edge_sem,
    ) = refs[10:]
    sp = lax.axis_index("sp")
    tp = lax.axis_index("tp")
    core = lax.rem(tp, CORES)
    mate = tp + 1 - 2 * core
    chips = tp_count // CORES
    targets = sp_count // CORES
    share = targets // head_count
    rows, features = tokens_ref.shape
    chunks = rows // chunk
    half = chunk // 2
    width = head_count * head_dim
    order = [chunks - 1] + list(range(chunks - 1))

    loads = [
        pltpu.make_async_copy(ref, weights.at[index], weight_sem.at[index])
        for index, ref in enumerate(weight_refs)
    ]
    for load in loads:
        load.start()
    mine = pltpu.make_async_copy(tokens_ref, gathered.at[tp], own_sem)
    mine.start()
    padded[0:8, :] = jnp.zeros((8, width), jnp.float32)
    greet(
        [(lax.rem(sp + step, sp_count), tp) for step in range(1, sp_count)]
        + [(sp, mate)]
        + [(sp, lax.rem(tp + CORES * step, tp_count)) for step in range(1, chips)]
    )

    def block(number):
        return pl.ds(number * chunk, chunk)

    def to_mate(number):
        return mesh_copy(
            tokens_ref.at[block(number)], gathered.at[tp, block(number)], mate_send.at[number],
            tok_recv.at[tp, number], (sp, mate),
        )

    def across(step, number):
        return mesh_copy(
            tokens_ref.at[block(number)], gathered.at[tp, block(number)],
            cross_send.at[step - 1, number], tok_recv.at[tp, number],
            (sp, lax.rem(tp + CORES * step, tp_count)),
        )

    def token_pass(step, number):
        other = lax.rem(tp + CORES * step, tp_count)
        return mesh_copy(
            gathered.at[other, block(number)], gathered.at[other, block(number)],
            tok_pass_send.at[step - 1, number], tok_recv.at[other, number], (sp, mate),
        )

    def token_arrival(source, number):
        return mesh_copy(
            tokens_ref.at[block(number)], gathered.at[source, block(number)], mate_send.at[number],
            tok_recv.at[source, number], (sp, mate),
        )

    for number in order:
        for step in range(1, chips):
            across(step, number).start()
        to_mate(number).start()

    owner = core == sp // targets

    def target_of(step):
        at = lax.rem(sp + 1 + step, targets)
        return at // share, core * targets + at

    def side_copy(step, head, target):
        return mesh_copy(
            side_ref.at[head], side_out.at[sp], side_ssem.at[step], side_rsem.at[sp], (target, tp)
        )

    def kv_copy(step, number, head, target):
        return mesh_copy(
            kv_send.at[head, block(number)], kv_out.at[sp, block(number)],
            kv_ssem.at[step, number], kv_rsem.at[sp, number], (target, tp),
        )

    def query_copy(step, number, head, target):
        at = pl.ds(number * half, half)
        return mesh_copy(
            query_send.at[head, at], query_out.at[sp, at],
            query_ssem.at[step, number], query_rsem.at[sp, number], (target, tp),
        )

    def kept(number, head):
        at = pl.ds(number * half, half)
        return (
            pltpu.make_async_copy(
                kv_send.at[head, block(number)], kv_out.at[sp, block(number)], local.at[0, number]
            ),
            pltpu.make_async_copy(
                query_send.at[head, at], query_out.at[sp, at], local.at[1, number]
            ),
        )

    def kept_side(head):
        return pltpu.make_async_copy(side_ref.at[head], side_out.at[sp], local.at[2, 0])

    for step in range(targets):
        head, target = target_of(step)

        @pl.when(target != sp)
        def _():
            side_copy(step, head, target).start()

        @pl.when(target == sp)
        def _():
            kept_side(head).start()

    ones_row = lax.broadcasted_iota(jnp.int32, (width, width), 0) // head_dim
    ones_column = lax.broadcasted_iota(jnp.int32, (width, width), 1) // head_dim
    spread = jnp.where(ones_row == ones_column, 1.0 / head_dim, 0.0).astype(jnp.bfloat16)

    def normed(values, gain):
        squares = values * values
        high = squares.astype(jnp.bfloat16)
        low = (squares - high.astype(jnp.float32)).astype(jnp.bfloat16)
        mean = jnp.dot(high, spread, preferred_element_type=jnp.float32)
        mean = mean + jnp.dot(low, spread, preferred_element_type=jnp.float32)
        return values * lax.rsqrt(mean + NORM_EPSILON) * gain

    mine.wait()
    for load in loads:
        load.wait()
    for number in order:
        here = block(number)
        for step in range(1, chips):
            token_arrival(lax.rem(tp + CORES * step, tp_count), number).wait_recv()
            token_pass(step, number).start()
        token_arrival(mate, number).wait_recv()
        for step in range(1, chips):
            token_arrival(lax.rem(mate + CORES * step, tp_count), number).wait_recv()
        total = jnp.zeros((chunk, 1), jnp.float32)
        for source in range(tp_count):
            part = gathered[source, here, :].astype(jnp.float32)
            at = slice(source * features, (source + 1) * features)
            total = total + jnp.sum(part * part, axis=1, keepdims=True)
            scaled[:, at] = (part * mix_ref[:, at]).astype(jnp.bfloat16)
        row_scale = lax.rsqrt(total / (tp_count * features) + NORM_EPSILON)

        def project(index):
            product = jnp.dot(scaled[...], weights[index], preferred_element_type=jnp.float32)
            return product * row_scale

        keys = normed(project(1), qkv_gain_ref[1:2, :]).astype(jnp.bfloat16)
        values = project(2).astype(jnp.bfloat16)
        queries = normed(project(0), qkv_gain_ref[0:1, :]).astype(jnp.bfloat16)
        queries = (queries.astype(jnp.float32) * head_dim ** (-0.5)).astype(jnp.bfloat16)
        for head in range(head_count):
            at = slice(head * head_dim, (head + 1) * head_dim)
            kv_send[head, here, :] = jnp.concatenate([keys[:, at], values[:, at]], axis=1)
            query_send[head, pl.ds(number * half, half), :] = jnp.concatenate(
                [queries[:half, at], queries[half:, at]], axis=1
            )
        for step in range(targets):
            head, target = target_of(step)

            @pl.when(target != sp)
            def _():
                kv_copy(step, number, head, target).start()
                query_copy(step, number, head, target).start()

            @pl.when(target == sp)
            def _():
                for copy in kept(number, head):
                    copy.start()

        outer[here, :] = project(3)
        gated = (project(4) * project(5)).astype(jnp.bfloat16)
        padded[pl.ds(8 + number * chunk, chunk), :] = gated.astype(jnp.float32)
        if number == chunks - 1:
            edge_send[...] = gated[chunk - 16 :, :]

            @pl.when(sp < sp_count - 1)
            def _():
                mesh_copy(
                    edge_send, edge_recv, edge_sem.at[0], edge_sem.at[1],
                    (lax.rem(sp + 1, sp_count), tp),
                ).start()

    edge = mesh_copy(
        edge_send, edge_recv, edge_sem.at[0], edge_sem.at[1], (lax.rem(sp + 1, sp_count), tp)
    )

    @pl.when(sp > 0)
    def _():
        edge.wait_recv()
        padded[0:8, :] = edge_recv[8:16, :].astype(jnp.float32)

    taps = taps_ref.shape[0]
    for number in range(chunks):
        convolved = jnp.zeros((chunk, width), jnp.float32)
        for tap in range(taps):
            at = pl.ds(8 - taps + 1 + tap + number * chunk, chunk)
            convolved = convolved + taps_ref[tap : tap + 1, :] * padded[at, :]
        conv_out[block(number), :] = normed(
            outer[block(number), :] * convolved, conv_gain_ref[...]
        ).astype(jnp.bfloat16)

    def kv_pass(source, number):
        return mesh_copy(
            kv_out.at[source, block(number)], kv_out.at[source, block(number)],
            kv_psem.at[source, number], kv_prsem.at[source, number], (sp, mate),
        )

    def query_pass(source, number):
        at = pl.ds(number * half, half)
        return mesh_copy(
            query_out.at[source, at], query_out.at[source, at],
            query_psem.at[source, number], query_prsem.at[source, number], (sp, mate),
        )

    def side_pass(source):
        return mesh_copy(
            side_out.at[source], side_out.at[source], side_psem.at[source], side_prsem.at[source],
            (sp, mate),
        )

    sources = [lax.rem(sp + step, sp_count) for step in range(sp_count)]

    @pl.when(owner)
    def _():
        for step, source in enumerate(sources):
            if step == 0:
                kept_side(0).wait()
            else:
                mesh_copy(
                    side_ref.at[0], side_out.at[source], side_ssem.at[0], side_rsem.at[source],
                    (sp, mate),
                ).wait_recv()
            side_pass(source).start()
        for number in order:
            at = pl.ds(number * half, half)
            for step, source in enumerate(sources):
                if step == 0:
                    for copy in kept(number, 0):
                        copy.wait()
                else:
                    mesh_copy(
                        kv_send.at[0, block(number)], kv_out.at[source, block(number)],
                        kv_ssem.at[0, number], kv_rsem.at[source, number], (sp, mate),
                    ).wait_recv()
                    mesh_copy(
                        query_send.at[0, at], query_out.at[source, at],
                        query_ssem.at[0, number], query_rsem.at[source, number], (sp, mate),
                    ).wait_recv()
                kv_pass(source, number).start()
                query_pass(source, number).start()
        for source in sources:
            side_pass(source).wait_send()
            for number in order:
                kv_pass(source, number).wait_send()
                query_pass(source, number).wait_send()

    @pl.when(jnp.logical_not(owner))
    def _():
        for source in sources:
            side_pass(source).wait_recv()
            for number in order:
                kv_pass(source, number).wait_recv()
                query_pass(source, number).wait_recv()

    for step in range(targets):
        head, target = target_of(step)

        @pl.when(target != sp)
        def _():
            side_copy(step, head, target).wait_send()
            for number in order:
                kv_copy(step, number, head, target).wait_send()
                query_copy(step, number, head, target).wait_send()

    for number in order:
        to_mate(number).wait_send()
        for step in range(1, chips):
            across(step, number).wait_send()
            token_pass(step, number).wait_send()

    @pl.when(sp < sp_count - 1)
    def _():
        edge.wait_send()


def front(tokens, mix_gain, qkv_gain, taps, conv_gain, sides, weights, head_dim, piece):
    sp_count = lax.axis_size("sp")
    tp_count = lax.axis_size("tp")
    rows, features = tokens.shape
    width = weights[0].shape[1]
    heads = width // head_dim
    chunk = min(256, piece)
    chunks = rows // chunk
    chips = tp_count // CORES
    targets = sp_count // CORES
    bf16 = jnp.bfloat16
    dma = pltpu.SemaphoreType.DMA
    across = (max(chips - 1, 1), chunks)
    vmem = pl.BlockSpec(memory_space=VMEM)
    return pl.pallas_call(
        functools.partial(front_kernel, (sp_count, tp_count, heads, head_dim, chunk)),
        out_shape=(
            jax.ShapeDtypeStruct((sp_count, rows, LANES), bf16),
            jax.ShapeDtypeStruct((sp_count, rows // 2, LANES), bf16),
            jax.ShapeDtypeStruct((sp_count,) + sides.shape[1:], sides.dtype),
            jax.ShapeDtypeStruct((rows, width), bf16),
        ),
        in_specs=[vmem] * 6 + [pl.BlockSpec(memory_space=pl.ANY)] * 6,
        out_specs=(vmem,) * 4,
        scratch_shapes=[
            VMEM((6,) + weights[0].shape, bf16),
            VMEM((tp_count, rows, features), bf16),
            VMEM((chunk, tp_count * features), bf16),
            VMEM((heads, rows, LANES), bf16),
            VMEM((heads, rows // 2, LANES), bf16),
            VMEM((rows, width), jnp.float32),
            VMEM((rows + 8, width), jnp.float32),
            VMEM((16, width), bf16),
            VMEM((16, width), bf16),
            dma((6,)), dma, dma(across), dma((chunks,)), dma(across), dma((tp_count, chunks)),
            dma((targets, chunks)), dma((sp_count, chunks)),
            dma((targets, chunks)), dma((sp_count, chunks)),
            dma((targets,)), dma((sp_count,)),
            dma((sp_count, chunks)), dma((sp_count, chunks)),
            dma((sp_count, chunks)), dma((sp_count, chunks)),
            dma((sp_count,)), dma((sp_count,)),
            dma((3, chunks)), dma((2,)),
        ],
        compiler_params=pltpu.CompilerParams(
            collective_id=0, has_side_effects=True, vmem_limit_bytes=56 * 1024 * 1024
        ),
    )(tokens, mix_gain, qkv_gain, taps, conv_gain, sides, *weights)


def back_kernel(
    plan, done_ref, conv_ref, attn_weight, conv_weight, out_ref, landed, attn, partial, keep,
    mate_out, mate_in, link_out, link_in, send, recv, local, mate_ssem, mate_rsem, link_ssem,
    link_rsem
):
    sp_count, tp_count, head_dim, sub = plan
    sp = lax.axis_index("sp")
    tp = lax.axis_index("tp")
    core = lax.rem(tp, CORES)
    mate = tp + 1 - 2 * core
    chips = tp_count // CORES
    first = tp - core
    targets = sp_count // CORES
    rows, width = conv_ref.shape
    half = done_ref.shape[1]
    piece = 2 * half
    pieces = rows // piece
    share = pieces // CORES
    block_rows = rows // tp_count
    subs = block_rows // sub
    greet(
        [
            (lax.rem(sp + step, sp_count), first + lax.rem(core + other, CORES))
            for step in range(sp_count)
            for other in range(CORES)
            if step or other
        ]
        + [(sp, lax.rem(tp + CORES * step, tp_count)) for step in range(1, chips)]
    )
    home = sp // targets
    slot = lax.rem(sp, targets) * CORES + core
    home_here = home == core

    def away(step):
        source = lax.rem(sp + step, sp_count)
        return mesh_copy(
            done_ref.at[source], landed.at[slot], send.at[step], recv.at[slot],
            (source, first + home),
        )

    for step in range(1, sp_count):
        away(step).start()

    @pl.when(home_here)
    def _():
        pltpu.make_async_copy(done_ref.at[sp], landed.at[slot], local).start()

    @pl.when(jnp.logical_not(home_here))
    def _():
        away(0).start()

    for number in range(rows // block_rows):
        at = pl.ds(number * block_rows, block_rows)
        partial[at, :] = jnp.dot(
            conv_ref[at, :], conv_weight[...], preferred_element_type=jnp.float32
        )

    for index in range(targets * CORES):
        giver = core * targets + index // CORES
        here = jnp.logical_and(giver == sp, core == index % CORES)

        @pl.when(here)
        def _():
            pltpu.make_async_copy(done_ref.at[0], landed.at[index], local).wait()

        @pl.when(jnp.logical_not(here))
        def _():
            mesh_copy(
                done_ref.at[0], landed.at[index], send.at[0], recv.at[index], (sp, mate)
            ).wait_recv()

        head = index // (share * CORES)
        place = index % (share * CORES)
        spot = jnp.where(lax.rem(sp, 2) == 0, place, pieces - 1 - place)
        start = pl.multiple_of(spot * piece, piece)
        lanes = slice(head * head_dim, (head + 1) * head_dim)
        attn[pl.ds(start, half), lanes] = landed[index, :, :head_dim]
        attn[pl.ds(start + half, half), lanes] = landed[index, :, head_dim:]

    def product(block, number):
        at = pl.ds(pl.multiple_of(block * block_rows + number * sub, sub), sub)
        return partial[at, :] + jnp.dot(
            attn[at, :], attn_weight[...], preferred_element_type=jnp.float32
        )

    def within(number):
        return pl.ds(number * sub, sub)

    def to_mate(step, number):
        at = within(number)
        return mesh_copy(
            mate_out.at[step, at], mate_in.at[step, at], mate_ssem.at[step, number],
            mate_rsem.at[step, number], (sp, mate),
        )

    def across(step, number):
        at = within(number)
        return mesh_copy(
            link_out.at[step - 1, at], link_in.at[step - 1, at], link_ssem.at[step - 1, number],
            link_rsem.at[step - 1, number], (sp, lax.rem(tp + CORES * step, tp_count)),
        )

    def joined(step, number):
        at = within(number)
        to_mate(step, number).wait_recv()
        total = keep[step, at, :] + mate_in[step, at, :].astype(jnp.float32)
        link_out[step - 1, at, :] = total.astype(jnp.bfloat16)
        across(step, number).start()

    waiting = []
    for step in list(range(1, chips)) + [0]:
        for number in range(subs):
            at = within(number)
            theirs = lax.rem(mate + CORES * step, tp_count)
            ours = lax.rem(tp + CORES * step, tp_count)
            mate_out[step, at, :] = product(theirs, number).astype(jnp.bfloat16)
            to_mate(step, number).start()
            keep[step, at, :] = product(ours, number)
            if waiting:
                joined(*waiting.pop())
            if step:
                waiting.append((step, number))
    for number in range(subs):
        at = within(number)
        to_mate(0, number).wait_recv()
        total = keep[0, at, :] + mate_in[0, at, :].astype(jnp.float32)
        for step in range(1, chips):
            across(step, number).wait_recv()
            total = total + link_in[step - 1, at, :].astype(jnp.float32)
        out_ref[at, :] = total.astype(jnp.bfloat16)
    for step in range(chips):
        for number in range(subs):
            to_mate(step, number).wait_send()
            if step:
                across(step, number).wait_send()
    for step in range(1, sp_count):
        away(step).wait_send()

    @pl.when(jnp.logical_not(home_here))
    def _():
        away(0).wait_send()


def back(done, conv_mixed, attn_weight, conv_weight, head_dim):
    sp_count = lax.axis_size("sp")
    tp_count = lax.axis_size("tp")
    chips = tp_count // CORES
    rows, width = conv_mixed.shape
    features = attn_weight.shape[1]
    block_rows = rows // tp_count
    sub = min(64, block_rows)
    subs = block_rows // sub
    links = max(chips - 1, 1)
    bf16 = jnp.bfloat16
    dma = pltpu.SemaphoreType.DMA
    vmem = pl.BlockSpec(memory_space=VMEM)
    return pl.pallas_call(
        functools.partial(back_kernel, (sp_count, tp_count, head_dim, sub)),
        out_shape=jax.ShapeDtypeStruct((block_rows, features), bf16),
        in_specs=[vmem] * 4,
        out_specs=vmem,
        scratch_shapes=[
            VMEM(done.shape, bf16),
            VMEM((rows, width), bf16),
            VMEM((rows, features), jnp.float32),
            VMEM((chips, block_rows, features), jnp.float32),
            VMEM((chips, block_rows, features), bf16),
            VMEM((chips, block_rows, features), bf16),
            VMEM((links, block_rows, features), bf16),
            VMEM((links, block_rows, features), bf16),
            dma((sp_count,)), dma((sp_count,)), dma,
            dma((chips, subs)), dma((chips, subs)), dma((links, subs)), dma((links, subs)),
        ],
        compiler_params=pltpu.CompilerParams(
            collective_id=1, has_side_effects=True, vmem_limit_bytes=48 * 1024 * 1024
        ),
    )(done, conv_mixed, attn_weight, conv_weight)


def attention_kernel(begin_ref, query_ref, kv_ref, side_ref, out_ref):
    piece_rows = out_ref.shape[1] * 2
    head_dim = LANES // 2
    tile = min(256, piece_rows)
    half = tile // 2
    sub = 256
    full = pl.program_id(0)
    begin = pl.multiple_of(begin_ref[full], half)
    rows = kv_ref.shape[1]
    low = lax.broadcasted_iota(jnp.int32, (half, LANES), 1) < head_dim
    tiles = []
    for number in range(piece_rows // tile):
        pair = query_ref[0, pl.ds(begin + number * half, half), :].astype(jnp.float32)
        left = jnp.where(low, pair, 0.0)
        right = jnp.where(low, pltpu.roll(pair, head_dim, 1), 0.0)
        tiles.append(jnp.concatenate([left, right], axis=0).astype(jnp.bfloat16))

    def fold(source, carried, masked):
        results = []
        for number, (top, total) in enumerate(carried):
            scores = []
            new_top = top
            for start in range(0, rows, sub):
                gates = side_ref[source, start // LANES : (start + sub) // LANES, :]
                gate_row = jnp.concatenate(
                    [gates[row : row + 1, :] for row in range(sub // LANES)], axis=1
                )
                part = lax.dot_general(
                    tiles[number], kv_ref[source, start : start + sub, :],
                    (((1,), (1,)), ((), ())), preferred_element_type=jnp.float32,
                ) - gate_row
                if masked:
                    row = lax.broadcasted_iota(jnp.int32, part.shape, 0) + 2 * begin + number * tile
                    column = lax.broadcasted_iota(jnp.int32, part.shape, 1) + start
                    part = jnp.where(column <= row, part, -jnp.inf)
                new_top = jnp.maximum(new_top, jnp.max(part, axis=1, keepdims=True))
                scores.append(part)
            total = total * jnp.exp(top - new_top)
            for index, part in enumerate(scores):
                weights = jnp.exp(part - new_top).astype(jnp.bfloat16)
                total = total + jnp.dot(
                    weights, kv_ref[source, index * sub : (index + 1) * sub, :],
                    preferred_element_type=jnp.float32,
                )
            results.append((new_top, total))
        return tuple(results)

    carried = tuple(
        (jnp.full((tile, 1), -1e30, jnp.float32), jnp.zeros((tile, LANES), jnp.float32))
        for _ in tiles
    )
    carried = lax.fori_loop(0, full, lambda index, now: fold(index, now, False), carried)
    carried = fold(full, carried, True)
    gain = side_ref[0, rows // LANES : rows // LANES + 1, :head_dim]
    mixed = []
    for _, total in carried:
        attended = total[:, head_dim:]
        scale = lax.rsqrt(jnp.mean(attended * attended, axis=1, keepdims=True) + NORM_EPSILON)
        mixed.append((attended * scale * gain).astype(jnp.bfloat16))
    mixed = jnp.concatenate(mixed, axis=0)
    middle = piece_rows // 2
    out_ref[0] = jnp.concatenate([mixed[:middle], mixed[middle:]], axis=1)


def attention(begins, queries, kv, sides, piece):
    sp_count = queries.shape[0]
    return pl.pallas_call(
        attention_kernel,
        grid_spec=pltpu.PrefetchScalarGridSpec(
            num_scalar_prefetch=1,
            grid=(sp_count,),
            in_specs=[
                pl.BlockSpec((1,) + queries.shape[1:], lambda i, n: (i, 0, 0)),
                pl.BlockSpec(kv.shape, lambda i, n: (0, 0, 0)),
                pl.BlockSpec(sides.shape, lambda i, n: (0, 0, 0)),
            ],
            out_specs=pl.BlockSpec((1, piece // 2, LANES), lambda i, n: (i, 0, 0)),
        ),
        out_shape=jax.ShapeDtypeStruct((sp_count, piece // 2, LANES), jnp.bfloat16),
        compiler_params=pltpu.CompilerParams(vmem_limit_bytes=48 * 1024 * 1024),
    )(begins, queries, kv, sides)


def per_device(
    tokens,
    mix_gain,
    query_weight,
    key_weight,
    value_weight,
    outer_gate_weight,
    inner_gate_weight,
    conv_input_weight,
    query_gain,
    key_gain,
    gate_totals,
    conv_taps,
    attn_out_gain,
    conv_out_gain,
    attn_out_weight,
    conv_out_weight,
):
    rows = tokens.shape[0]
    head_dim = query_gain.shape[0]
    width = query_weight.shape[1]
    heads = width // head_dim
    sp = lax.axis_index("sp")
    sp_count = lax.axis_size("sp")
    core = lax.rem(lax.axis_index("tp"), CORES)
    share = sp_count // CORES // heads
    pieces = CORES * share
    piece = rows // pieces
    gate_rows = gate_totals.T.reshape(heads, rows // LANES, LANES)
    gain_rows = jnp.pad(
        attn_out_gain.reshape(heads, 1, head_dim), ((0, 0), (0, 7), (0, LANES - head_dim))
    )
    sides = jnp.concatenate([gate_rows, gain_rows], axis=1)
    qkv_gain = jnp.stack([jnp.tile(query_gain, heads), jnp.tile(key_gain, heads)])
    kv, queries, sides, conv_mixed = front(
        tokens,
        mix_gain.reshape(1, -1),
        qkv_gain,
        conv_taps,
        conv_out_gain.reshape(1, -1),
        sides,
        (
            query_weight,
            key_weight,
            value_weight,
            outer_gate_weight,
            inner_gate_weight,
            conv_input_weight,
        ),
        head_dim,
        piece,
    )
    place = lax.rem(sp, share) * CORES + core
    source = jnp.arange(sp_count, dtype=jnp.int32)
    spot = jnp.where(source % 2 == 0, place, pieces - 1 - place)
    begins = (spot * (piece // 2)).astype(jnp.int32)
    finished = attention(begins, queries, kv, sides, piece)
    return back(finished, conv_mixed, attn_out_weight, conv_out_weight, head_dim)


def solution(mesh):
    placed = (
        P("sp", "tp"),
        P(),
        P(None, "tp"),
        P(None, "tp"),
        P(None, "tp"),
        P(None, "tp"),
        P(None, "tp"),
        P(None, "tp"),
        P(),
        P(),
        P("sp", "tp"),
        P(None, "tp"),
        P("tp"),
        P("tp"),
        P("tp", None),
        P("tp", None),
    )
    return jax.shard_map(
        per_device, mesh=mesh, in_specs=placed, out_specs=P(("sp", "tp"), None), check_vma=False
    )
```

```python
import functools

import jax
import jax.numpy as jnp
from jax import lax
from jax.experimental import pallas as pl
from jax.experimental.pallas import tpu as pltpu
from jax.sharding import PartitionSpec as P

NORM_EPSILON = 1e-06
MESH = pl.DeviceIdType.MESH
CORES = 2
LANES = 128
VMEM = pltpu.VMEM


def greet(devices):
    barrier = pltpu.get_barrier_semaphore()
    for sp, tp in devices:
        pl.semaphore_signal(barrier, inc=1, device_id=(sp, tp), device_id_type=MESH)
    pl.semaphore_wait(barrier, len(devices))


def mesh_copy(src, dst, send, recv, device):
    return pltpu.make_async_remote_copy(
        src, dst, send, recv, device_id=device, device_id_type=MESH
    )


def front_kernel(
    plan, tokens_ref, mix_ref, query_gain_ref, key_gain_ref, taps_ref, conv_gain_ref, side_ref, *refs
):
    sp_count, tp_count, head_count, head_dim, chunk = plan
    query_gain = jnp.concatenate([query_gain_ref[...]] * plan[2], axis=1)
    key_gain = jnp.concatenate([key_gain_ref[...]] * plan[2], axis=1)
    weight_refs = refs[:6]
    kv_out, query_out, side_out, conv_out = refs[6:10]
    (
        weights, gathered, scaled, kv_send, query_send, outer, padded, edge_send, edge_recv,
        weight_sem, own_sem, cross_send, mate_send, tok_pass_send, tok_recv,
        kv_ssem, kv_rsem, query_ssem, query_rsem, side_ssem, side_rsem,
        kv_psem, kv_prsem, query_psem, query_prsem, side_psem, side_prsem, local, edge_sem,
    ) = refs[10:]
    sp = lax.axis_index("sp")
    tp = lax.axis_index("tp")
    core = lax.rem(tp, CORES)
    mate = tp + 1 - 2 * core
    chips = tp_count // CORES
    targets = sp_count // CORES
    share = targets // head_count
    rows, features = tokens_ref.shape
    chunks = rows // chunk
    half = chunk // 2
    width = head_count * head_dim
    order = [chunks - 1] + list(range(chunks - 1))

    loads = [
        pltpu.make_async_copy(ref, weights.at[index], weight_sem.at[index])
        for index, ref in enumerate(weight_refs)
    ]
    for load in loads:
        load.start()
    mine = pltpu.make_async_copy(tokens_ref, gathered.at[tp], own_sem)
    mine.start()
    padded[0:8, :] = jnp.zeros((8, width), jnp.float32)
    greet(
        [(lax.rem(sp + step, sp_count), tp) for step in range(1, sp_count)]
        + [(sp, mate)]
        + [(sp, lax.rem(tp + CORES * step, tp_count)) for step in range(1, chips)]
    )

    def block(number):
        return pl.ds(number * chunk, chunk)

    def to_mate(number):
        return mesh_copy(
            tokens_ref.at[block(number)], gathered.at[tp, block(number)], mate_send.at[number],
            tok_recv.at[tp, number], (sp, mate),
        )

    def across(step, number):
        return mesh_copy(
            tokens_ref.at[block(number)], gathered.at[tp, block(number)],
            cross_send.at[step - 1, number], tok_recv.at[tp, number],
            (sp, lax.rem(tp + CORES * step, tp_count)),
        )

    def token_pass(step, number):
        other = lax.rem(tp + CORES * step, tp_count)
        return mesh_copy(
            gathered.at[other, block(number)], gathered.at[other, block(number)],
            tok_pass_send.at[step - 1, number], tok_recv.at[other, number], (sp, mate),
        )

    def token_arrival(source, number):
        return mesh_copy(
            tokens_ref.at[block(number)], gathered.at[source, block(number)], mate_send.at[number],
            tok_recv.at[source, number], (sp, mate),
        )

    for number in order:
        for step in range(1, chips):
            across(step, number).start()
        to_mate(number).start()

    owner = core == sp // targets

    def target_of(step):
        at = lax.rem(sp + 1 + step, targets)
        return at // share, core * targets + at

    def side_copy(step, head, target):
        return mesh_copy(
            side_ref.at[head], side_out.at[sp], side_ssem.at[step], side_rsem.at[sp], (target, tp)
        )

    def kv_copy(step, number, head, target):
        return mesh_copy(
            kv_send.at[head, block(number)], kv_out.at[sp, block(number)],
            kv_ssem.at[step, number], kv_rsem.at[sp, number], (target, tp),
        )

    def query_copy(step, number, head, target):
        at = pl.ds(number * half, half)
        return mesh_copy(
            query_send.at[head, at], query_out.at[sp, at],
            query_ssem.at[step, number], query_rsem.at[sp, number], (target, tp),
        )

    def kept(number, head):
        at = pl.ds(number * half, half)
        return (
            pltpu.make_async_copy(
                kv_send.at[head, block(number)], kv_out.at[sp, block(number)], local.at[0, number]
            ),
            pltpu.make_async_copy(
                query_send.at[head, at], query_out.at[sp, at], local.at[1, number]
            ),
        )

    def kept_side(head):
        return pltpu.make_async_copy(side_ref.at[head], side_out.at[sp], local.at[2, 0])

    for step in range(targets):
        head, target = target_of(step)

        @pl.when(target != sp)
        def _():
            side_copy(step, head, target).start()

        @pl.when(target == sp)
        def _():
            kept_side(head).start()

    ones_row = lax.broadcasted_iota(jnp.int32, (width, width), 0) // head_dim
    ones_column = lax.broadcasted_iota(jnp.int32, (width, width), 1) // head_dim
    spread = jnp.where(ones_row == ones_column, 1.0 / head_dim, 0.0).astype(jnp.bfloat16)

    def normed(values, gain):
        squares = values * values
        high = squares.astype(jnp.bfloat16)
        low = (squares - high.astype(jnp.float32)).astype(jnp.bfloat16)
        mean = jnp.dot(high, spread, preferred_element_type=jnp.float32)
        mean = mean + jnp.dot(low, spread, preferred_element_type=jnp.float32)
        return values * lax.rsqrt(mean + NORM_EPSILON) * gain

    mine.wait()
    for load in loads:
        load.wait()
    for number in order:
        here = block(number)
        for step in range(1, chips):
            token_arrival(lax.rem(tp + CORES * step, tp_count), number).wait_recv()
            token_pass(step, number).start()
        token_arrival(mate, number).wait_recv()
        for step in range(1, chips):
            token_arrival(lax.rem(mate + CORES * step, tp_count), number).wait_recv()
        total = jnp.zeros((chunk, 1), jnp.float32)
        for source in range(tp_count):
            part = gathered[source, here, :].astype(jnp.float32)
            at = slice(source * features, (source + 1) * features)
            total = total + jnp.sum(part * part, axis=1, keepdims=True)
            scaled[:, at] = (part * mix_ref[:, at]).astype(jnp.bfloat16)
        row_scale = lax.rsqrt(total / (tp_count * features) + NORM_EPSILON)

        def project(index):
            product = jnp.dot(scaled[...], weights[index], preferred_element_type=jnp.float32)
            return product * row_scale

        keys = normed(project(1), key_gain).astype(jnp.bfloat16)
        values = project(2).astype(jnp.bfloat16)
        queries = normed(project(0), query_gain).astype(jnp.bfloat16)
        queries = (queries.astype(jnp.float32) * head_dim ** (-0.5)).astype(jnp.bfloat16)
        for head in range(head_count):
            at = slice(head * head_dim, (head + 1) * head_dim)
            kv_send[head, here, :] = jnp.concatenate([keys[:, at], values[:, at]], axis=1)
            query_send[head, pl.ds(number * half, half), :] = jnp.concatenate(
                [queries[:half, at], queries[half:, at]], axis=1
            )
        for step in range(targets):
            head, target = target_of(step)

            @pl.when(target != sp)
            def _():
                kv_copy(step, number, head, target).start()
                query_copy(step, number, head, target).start()

            @pl.when(target == sp)
            def _():
                for copy in kept(number, head):
                    copy.start()

        outer[here, :] = project(3)
        gated = (project(4) * project(5)).astype(jnp.bfloat16)
        padded[pl.ds(8 + number * chunk, chunk), :] = gated.astype(jnp.float32)
        if number == chunks - 1:
            edge_send[...] = gated[chunk - 16 :, :]

            @pl.when(sp < sp_count - 1)
            def _():
                mesh_copy(
                    edge_send, edge_recv, edge_sem.at[0], edge_sem.at[1],
                    (lax.rem(sp + 1, sp_count), tp),
                ).start()

    edge = mesh_copy(
        edge_send, edge_recv, edge_sem.at[0], edge_sem.at[1], (lax.rem(sp + 1, sp_count), tp)
    )

    @pl.when(sp > 0)
    def _():
        edge.wait_recv()
        padded[0:8, :] = edge_recv[8:16, :].astype(jnp.float32)

    taps = taps_ref.shape[0]
    for number in range(chunks):
        convolved = jnp.zeros((chunk, width), jnp.float32)
        for tap in range(taps):
            at = pl.ds(8 - taps + 1 + tap + number * chunk, chunk)
            convolved = convolved + taps_ref[tap : tap + 1, :] * padded[at, :]
        conv_out[block(number), :] = normed(
            outer[block(number), :] * convolved, conv_gain_ref[...]
        ).astype(jnp.bfloat16)

    def kv_pass(source, number):
        return mesh_copy(
            kv_out.at[source, block(number)], kv_out.at[source, block(number)],
            kv_psem.at[source, number], kv_prsem.at[source, number], (sp, mate),
        )

    def query_pass(source, number):
        at = pl.ds(number * half, half)
        return mesh_copy(
            query_out.at[source, at], query_out.at[source, at],
            query_psem.at[source, number], query_prsem.at[source, number], (sp, mate),
        )

    def side_pass(source):
        return mesh_copy(
            side_out.at[source], side_out.at[source], side_psem.at[source], side_prsem.at[source],
            (sp, mate),
        )

    sources = [lax.rem(sp + step, sp_count) for step in range(sp_count)]

    @pl.when(owner)
    def _():
        for step, source in enumerate(sources):
            if step == 0:
                kept_side(0).wait()
            else:
                mesh_copy(
                    side_ref.at[0], side_out.at[source], side_ssem.at[0], side_rsem.at[source],
                    (sp, mate),
                ).wait_recv()
            side_pass(source).start()
        for number in order:
            at = pl.ds(number * half, half)
            for step, source in enumerate(sources):
                if step == 0:
                    for copy in kept(number, 0):
                        copy.wait()
                else:
                    mesh_copy(
                        kv_send.at[0, block(number)], kv_out.at[source, block(number)],
                        kv_ssem.at[0, number], kv_rsem.at[source, number], (sp, mate),
                    ).wait_recv()
                    mesh_copy(
                        query_send.at[0, at], query_out.at[source, at],
                        query_ssem.at[0, number], query_rsem.at[source, number], (sp, mate),
                    ).wait_recv()
                kv_pass(source, number).start()
                query_pass(source, number).start()
        for source in sources:
            side_pass(source).wait_send()
            for number in order:
                kv_pass(source, number).wait_send()
                query_pass(source, number).wait_send()

    @pl.when(jnp.logical_not(owner))
    def _():
        for source in sources:
            side_pass(source).wait_recv()
            for number in order:
                kv_pass(source, number).wait_recv()
                query_pass(source, number).wait_recv()

    for step in range(targets):
        head, target = target_of(step)

        @pl.when(target != sp)
        def _():
            side_copy(step, head, target).wait_send()
            for number in order:
                kv_copy(step, number, head, target).wait_send()
                query_copy(step, number, head, target).wait_send()

    for number in order:
        to_mate(number).wait_send()
        for step in range(1, chips):
            across(step, number).wait_send()
            token_pass(step, number).wait_send()

    @pl.when(sp < sp_count - 1)
    def _():
        edge.wait_send()


def front(tokens, mix_gain, query_gain, key_gain, taps, conv_gain, sides, weights, head_dim, piece):
    sp_count = lax.axis_size("sp")
    tp_count = lax.axis_size("tp")
    rows, features = tokens.shape
    width = weights[0].shape[1]
    heads = width // head_dim
    chunk = min(256, piece)
    chunks = rows // chunk
    chips = tp_count // CORES
    targets = sp_count // CORES
    bf16 = jnp.bfloat16
    dma = pltpu.SemaphoreType.DMA
    across = (max(chips - 1, 1), chunks)
    vmem = pl.BlockSpec(memory_space=VMEM)
    return pl.pallas_call(
        functools.partial(front_kernel, (sp_count, tp_count, heads, head_dim, chunk)),
        out_shape=(
            jax.ShapeDtypeStruct((sp_count, rows, LANES), bf16),
            jax.ShapeDtypeStruct((sp_count, rows // 2, LANES), bf16),
            jax.ShapeDtypeStruct((sp_count,) + sides.shape[1:], sides.dtype),
            jax.ShapeDtypeStruct((rows, width), bf16),
        ),
        in_specs=[vmem] * 7 + [pl.BlockSpec(memory_space=pl.ANY)] * 6,
        out_specs=(vmem,) * 4,
        scratch_shapes=[
            VMEM((6,) + weights[0].shape, bf16),
            VMEM((tp_count, rows, features), bf16),
            VMEM((chunk, tp_count * features), bf16),
            VMEM((heads, rows, LANES), bf16),
            VMEM((heads, rows // 2, LANES), bf16),
            VMEM((rows, width), jnp.float32),
            VMEM((rows + 8, width), jnp.float32),
            VMEM((16, width), bf16),
            VMEM((16, width), bf16),
            dma((6,)), dma, dma(across), dma((chunks,)), dma(across), dma((tp_count, chunks)),
            dma((targets, chunks)), dma((sp_count, chunks)),
            dma((targets, chunks)), dma((sp_count, chunks)),
            dma((targets,)), dma((sp_count,)),
            dma((sp_count, chunks)), dma((sp_count, chunks)),
            dma((sp_count, chunks)), dma((sp_count, chunks)),
            dma((sp_count,)), dma((sp_count,)),
            dma((3, chunks)), dma((2,)),
        ],
        compiler_params=pltpu.CompilerParams(
            collective_id=0, has_side_effects=True, vmem_limit_bytes=56 * 1024 * 1024
        ),
    )(tokens, mix_gain, query_gain, key_gain, taps, conv_gain, sides, *weights)


def rear_kernel(
    plan, query_ref, kv_ref, side_ref, conv_ref, attn_weight, conv_weight, out_ref, done, landed,
    attn, partial, keep, mate_out, mate_in, link_out, link_in, send, recv, local, mate_ssem,
    mate_rsem, link_ssem, link_rsem
):
    sp_count, tp_count, head_dim, piece, sub = plan
    sp = lax.axis_index("sp")
    tp = lax.axis_index("tp")
    core = lax.rem(tp, CORES)
    mate = tp + 1 - 2 * core
    chips = tp_count // CORES
    first = tp - core
    targets = sp_count // CORES
    rows, width = conv_ref.shape
    pieces = rows // piece
    share = pieces // CORES
    block_rows = rows // tp_count
    chunk = min(256, piece)
    half = chunk // 2
    tile = piece // 2
    span = 256
    phases = 2
    subs = block_rows // phases // sub
    greet(
        [
            (lax.rem(sp + step, sp_count), first + lax.rem(core + other, CORES))
            for step in range(sp_count)
            for other in range(CORES)
            if step or other
        ]
        + [(sp, lax.rem(tp + CORES * step, tp_count)) for step in range(1, chips)]
    )
    home = sp // targets
    slot = lax.rem(sp, targets) * CORES + core
    home_here = home == core
    place_here = lax.rem(sp, share) * CORES + core
    low = lax.broadcasted_iota(jnp.int32, (half, LANES), 1) < head_dim
    gain = side_ref[0, rows // LANES : rows // LANES + 1, :head_dim]

    def away(phase, source):
        return mesh_copy(
            done.at[phase, source], landed.at[phase, slot], send.at[phase, source],
            recv.at[phase, slot], (source, first + home),
        )

    def stay(phase, source, index):
        return pltpu.make_async_copy(
            done.at[phase, source], landed.at[phase, index], local.at[phase]
        )

    def queries_of(phase, source, spot):
        begin = pl.multiple_of(spot * tile, half)
        parts = []
        for number in range(piece // chunk):
            pair = query_ref[source, pl.ds(begin + number * half, half), :].astype(jnp.float32)
            if phase:
                pair = pltpu.roll(pair, head_dim, 1)
            parts.append(jnp.where(low, pair, 0.0))
        return jnp.concatenate(parts, axis=0).astype(jnp.bfloat16)

    def fold(phase, source, queries, carried, spot=None):
        top, total = carried
        new_top = top
        scores = []
        for start in range(0, rows, span):
            gates = side_ref[source, start // LANES : (start + span) // LANES, :]
            gate_row = jnp.concatenate(
                [gates[row : row + 1, :] for row in range(span // LANES)], axis=1
            )
            part = lax.dot_general(
                queries, kv_ref[source, start : start + span, :],
                (((1,), (1,)), ((), ())), preferred_element_type=jnp.float32,
            ) - gate_row
            if spot is not None:
                row = lax.broadcasted_iota(jnp.int32, part.shape, 0)
                row = row // half * chunk + lax.rem(row, half) + phase * half + spot * piece
                column = lax.broadcasted_iota(jnp.int32, part.shape, 1) + start
                part = jnp.where(column <= row, part, -jnp.inf)
            new_top = jnp.maximum(new_top, jnp.max(part, axis=1, keepdims=True))
            scores.append(part)
        total = total * jnp.exp(top - new_top)
        for index, part in enumerate(scores):
            weights = jnp.exp(part - new_top).astype(jnp.bfloat16)
            total = total + jnp.dot(
                weights, kv_ref[source, index * span : (index + 1) * span, :],
                preferred_element_type=jnp.float32,
            )
        return new_top, total

    def finish(phase, source, carried):
        attended = carried[1][:, head_dim:]
        scale = lax.rsqrt(jnp.mean(attended * attended, axis=1, keepdims=True) + NORM_EPSILON)
        mixed = (attended * scale * gain).astype(jnp.bfloat16)
        done[phase, source, :, :] = jnp.concatenate(
            [mixed[: tile // 2], mixed[tile // 2 :]], axis=1
        )
        stays = jnp.logical_and(source == sp, home_here)

        @pl.when(stays)
        def _():
            stay(phase, source, slot).start()

        @pl.when(jnp.logical_not(stays))
        def _():
            away(phase, source).start()

    def attend(phase):
        def pair_of_sources(pair, _):
            even, odd = 2 * pair, 2 * pair + 1
            even_spot, odd_spot = place_here, pieces - 1 - place_here
            even_queries = queries_of(phase, even, even_spot)
            odd_queries = queries_of(phase, odd, odd_spot)
            empty = (
                jnp.full((tile, 1), -1e30, jnp.float32),
                jnp.zeros((tile, LANES), jnp.float32),
            )

            def both(source, carried):
                return (
                    fold(phase, source, even_queries, carried[0]),
                    fold(phase, source, odd_queries, carried[1]),
                )

            even_state, odd_state = lax.fori_loop(0, even, both, (empty, empty))
            odd_state = fold(phase, even, odd_queries, odd_state)
            even_state = fold(phase, even, even_queries, even_state, even_spot)
            odd_state = fold(phase, odd, odd_queries, odd_state, odd_spot)
            finish(phase, even, even_state)
            finish(phase, odd, odd_state)
            return 0

        lax.fori_loop(0, sp_count // 2, pair_of_sources, 0)

    def arrive(phase):
        for index in range(targets * CORES):
            giver = core * targets + index // CORES
            here = jnp.logical_and(giver == sp, core == index % CORES)

            @pl.when(here)
            def _():
                stay(phase, 0, index).wait()

            @pl.when(jnp.logical_not(here))
            def _():
                mesh_copy(
                    done.at[phase, 0], landed.at[phase, index], send.at[phase, 0],
                    recv.at[phase, index], (sp, mate),
                ).wait_recv()

            head = index // (share * CORES)
            place = index % (share * CORES)
            spot = jnp.where(lax.rem(sp, 2) == 0, place, pieces - 1 - place)
            lanes = slice(head * head_dim, (head + 1) * head_dim)
            for side, at in enumerate((0, tile // 2)):
                offset = at // half * chunk + phase * half + at % half
                start = pl.multiple_of(spot * piece + offset, tile // 2)
                attn[pl.ds(start, tile // 2), lanes] = landed[
                    phase, index, :, side * head_dim : (side + 1) * head_dim
                ]

    def product(block, number):
        at = pl.ds(pl.multiple_of(block * block_rows + number * sub, sub), sub)
        return partial[at, :] + jnp.dot(
            attn[at, :], attn_weight[...], preferred_element_type=jnp.float32
        )

    def within(number):
        return pl.ds(number * sub, sub)

    def to_mate(step, number):
        at = within(number)
        return mesh_copy(
            mate_out.at[step, at], mate_in.at[step, at], mate_ssem.at[step, number],
            mate_rsem.at[step, number], (sp, mate),
        )

    def across(step, number):
        at = within(number)
        return mesh_copy(
            link_out.at[step - 1, at], link_in.at[step - 1, at], link_ssem.at[step - 1, number],
            link_rsem.at[step - 1, number], (sp, lax.rem(tp + CORES * step, tp_count)),
        )

    def joined(step, number):
        at = within(number)
        to_mate(step, number).wait_recv()
        total = keep[step, at, :] + mate_in[step, at, :].astype(jnp.float32)
        link_out[step - 1, at, :] = total.astype(jnp.bfloat16)
        across(step, number).start()

    def spread(phase):
        waiting = []
        for step in list(range(1, chips)) + [0]:
            for number in range(phase * subs, (phase + 1) * subs):
                at = within(number)
                theirs = lax.rem(mate + CORES * step, tp_count)
                ours = lax.rem(tp + CORES * step, tp_count)
                mate_out[step, at, :] = product(theirs, number).astype(jnp.bfloat16)
                to_mate(step, number).start()
                keep[step, at, :] = product(ours, number)
                if waiting:
                    joined(*waiting.pop())
                if step:
                    waiting.append((step, number))

    def settle(phase):
        for number in range(phase * subs, (phase + 1) * subs):
            at = within(number)
            to_mate(0, number).wait_recv()
            total = keep[0, at, :] + mate_in[0, at, :].astype(jnp.float32)
            for step in range(1, chips):
                across(step, number).wait_recv()
                total = total + link_in[step - 1, at, :].astype(jnp.float32)
            out_ref[at, :] = total.astype(jnp.bfloat16)

    attend(0)
    for number in range(tp_count):
        at = pl.ds(number * block_rows, block_rows)
        partial[at, :] = jnp.dot(
            conv_ref[at, :], conv_weight[...], preferred_element_type=jnp.float32
        )
    arrive(0)
    spread(0)
    attend(1)
    settle(0)
    arrive(1)
    spread(1)
    settle(1)
    for step in range(chips):
        for number in range(phases * subs):
            to_mate(step, number).wait_send()
            if step:
                across(step, number).wait_send()
    for phase in range(phases):
        for step in range(1, sp_count):
            away(phase, lax.rem(sp + step, sp_count)).wait_send()

        @pl.when(jnp.logical_not(home_here))
        def _():
            away(phase, sp).wait_send()


def rear(queries, kv, sides, conv_mixed, attn_weight, conv_weight, head_dim, piece):
    sp_count = lax.axis_size("sp")
    tp_count = lax.axis_size("tp")
    chips = tp_count // CORES
    rows, width = conv_mixed.shape
    features = attn_weight.shape[1]
    block_rows = rows // tp_count
    sub = min(64, block_rows // 2)
    subs = block_rows // sub
    links = max(chips - 1, 1)
    bf16 = jnp.bfloat16
    dma = pltpu.SemaphoreType.DMA
    vmem = pl.BlockSpec(memory_space=VMEM)
    return pl.pallas_call(
        functools.partial(rear_kernel, (sp_count, tp_count, head_dim, piece, sub)),
        out_shape=jax.ShapeDtypeStruct((block_rows, features), bf16),
        in_specs=[vmem] * 6,
        out_specs=vmem,
        scratch_shapes=[
            VMEM((2, sp_count, piece // 4, LANES), bf16),
            VMEM((2, sp_count, piece // 4, LANES), bf16),
            VMEM((rows, width), bf16),
            VMEM((rows, features), jnp.float32),
            VMEM((chips, block_rows, features), jnp.float32),
            VMEM((chips, block_rows, features), bf16),
            VMEM((chips, block_rows, features), bf16),
            VMEM((links, block_rows, features), bf16),
            VMEM((links, block_rows, features), bf16),
            dma((2, sp_count)), dma((2, sp_count)), dma((2,)),
            dma((chips, subs)), dma((chips, subs)), dma((links, subs)), dma((links, subs)),
        ],
        compiler_params=pltpu.CompilerParams(
            collective_id=1, has_side_effects=True, vmem_limit_bytes=56 * 1024 * 1024
        ),
    )(queries, kv, sides, conv_mixed, attn_weight, conv_weight)


def per_device(
    tokens,
    mix_gain,
    query_weight,
    key_weight,
    value_weight,
    outer_gate_weight,
    inner_gate_weight,
    conv_input_weight,
    query_gain,
    key_gain,
    gate_totals,
    conv_taps,
    attn_out_gain,
    conv_out_gain,
    attn_out_weight,
    conv_out_weight,
):
    rows = tokens.shape[0]
    head_dim = query_gain.shape[0]
    width = query_weight.shape[1]
    heads = width // head_dim
    sp_count = lax.axis_size("sp")
    share = sp_count // CORES // heads
    pieces = CORES * share
    piece = rows // pieces
    gate_rows = gate_totals.T.reshape(heads, rows // LANES, LANES)
    gain_rows = jnp.pad(
        attn_out_gain.reshape(heads, 1, head_dim), ((0, 0), (0, 7), (0, LANES - head_dim))
    )
    sides = jnp.concatenate([gate_rows, gain_rows], axis=1)
    kv, queries, sides, conv_mixed = front(
        tokens,
        mix_gain.reshape(1, -1),
        query_gain.reshape(1, -1),
        key_gain.reshape(1, -1),
        conv_taps,
        conv_out_gain.reshape(1, -1),
        sides,
        (
            query_weight,
            key_weight,
            value_weight,
            outer_gate_weight,
            inner_gate_weight,
            conv_input_weight,
        ),
        head_dim,
        piece,
    )
    return rear(
        queries, kv, sides, conv_mixed, attn_out_weight, conv_out_weight, head_dim, piece
    )


def solution(mesh):
    placed = (
        P("sp", "tp"),
        P(),
        P(None, "tp"),
        P(None, "tp"),
        P(None, "tp"),
        P(None, "tp"),
        P(None, "tp"),
        P(None, "tp"),
        P(),
        P(),
        P("sp", "tp"),
        P(None, "tp"),
        P("tp"),
        P("tp"),
        P("tp", None),
        P("tp", None),
    )
    return jax.shard_map(
        per_device, mesh=mesh, in_specs=placed, out_specs=P(("sp", "tp"), None), check_vma=False
    )
```
